512 devices in a mesh: fs: 128 (over z, y, core), tp: 4 (over x).
Axes of the slice: x: 4, y: 8, z: 8, core: 2. Of those that a mesh axis runs over, the one named last changes fastest.
Arguments:
- saved_input: bfloat16 [98304, 2048], P('fs'), may hold values from -24 to 24
- cot_inproj: bfloat16 [98304, 1024], P('fs', 'tp'), may hold values from -0.019042969 to 0.019042969
- cot_outproj: bfloat16 [98304, 1024], P('fs', 'tp'), may hold values from -0.019042969 to 0.019042969
- factor_inproj: bfloat16 [2048, 256], P('fs')
- factor_outproj: bfloat16 [2048, 256], P('fs')
- weight_inproj: float32 [2048, 1024], P('fs', 'tp'), may hold values from -0.125 to 0.125
- weight_outproj: float32 [2048, 1024], P('fs', 'tp'), may hold values from -0.125 to 0.125
- first_inproj: float32 [256, 1024], P('fs', 'tp'), may hold values from -6 to 6
- first_outproj: float32 [256, 1024], P('fs', 'tp'), may hold values from -6 to 6
- second_inproj: float32 [256, 1024], P('fs', 'tp'), may hold values from 0.25 to 4
- second_outproj: float32 [256, 1024], P('fs', 'tp'), may hold values from 0.25 to 4
Outputs:
- update_inproj: float32 [2048, 1024], P('fs', 'tp')
- update_outproj: float32 [2048, 1024], P('fs', 'tp')
- new_inproj: float32 [2048, 1024], P('fs', 'tp')
- new_outproj: float32 [2048, 1024], P('fs', 'tp')
- copy_inproj: bfloat16 [2048, 1024], P(None, 'tp')
- copy_outproj: bfloat16 [2048, 1024], P(None, 'tp')
- first_inproj_new: float32 [256, 1024], P('fs', 'tp')
- first_outproj_new: float32 [256, 1024], P('fs', 'tp')
- second_inproj_new: float32 [256, 1024], P('fs', 'tp')
- second_outproj_new: float32 [256, 1024], P('fs', 'tp')
The draws below stay inside these ranges and needn't reach their ends.
All inputs are finite; a program needn't handle non-finite values.
Results may differ from the reference program's by a relative error of at most 0.00045.
Values may be sent and summed in bfloat16 or wider, within the bound.
A program may use at most 64 MiB of HBM per device.

```python
import math
import jax
import jax.numpy as jnp
from jax import lax

D = 2048
RANK = 256
GN = 1024
TOKENS = 98304


def lowrank_draw(key):
    base = jax.random.normal(key, (D, RANK), jnp.float32)
    position = jnp.arange(D).astype(jnp.float32) / D
    scale = jnp.exp(jnp.log(10.0) * position) * 0.22 * D ** (-0.5)
    return (base * scale[:, None]).astype(jnp.bfloat16)


def draw_factor_inproj(key, part):
    return lowrank_draw(jax.random.fold_in(key, 11))


def draw_factor_outproj(key, part):
    return lowrank_draw(jax.random.fold_in(key, 12))


def raised(values, stream_key, source, target, shards_of, factor):
    owner, partner = [(jnp.arange(values.shape[dim]) // (values.shape[dim] // shards_of)).reshape([-1 if axis == dim else 1 for axis in range(values.ndim)]) for dim in (source, target)]
    chosen = jax.random.permutation(stream_key, shards_of)[partner]
    strong = (owner == chosen) | (owner == (partner + shards_of // 2) % shards_of)
    return jnp.where(strong, factor * values, values)


def levels(rng, shape, cuts, least, high):
    level = 1.0
    for axis_at, shards_of in cuts:
        draws = jax.random.uniform(jax.random.fold_in(jax.random.fold_in(rng, 6), axis_at), (shards_of,), jnp.float32, least / len(cuts), high / len(cuts))
        level = level * jnp.repeat(jnp.exp(draws), shape[axis_at] // shards_of).reshape((-1,) + (1,) * (len(shape) - 1 - axis_at))
    return level


def normal_values(key, dims, spread, most, cuts=(), kind=jnp.bfloat16):
    array = spread * jax.random.normal(key, dims, jnp.float32)
    if cuts:
        array = array * levels(key, dims, cuts, -0.22, 0.18)
    return jnp.clip(array, -most, most).astype(kind)


def gaussian_with(stream_key, shape, width, limit, split, heavy, kind=jnp.bfloat16):
    array = width * jax.random.normal(stream_key, shape, jnp.float32)
    if split:
        array = array * levels(stream_key, shape, split, -0.22, 0.18)
    return jnp.clip(raised(array, jax.random.fold_in(stream_key, 3), *heavy), -limit, limit).astype(kind)


def setup_inputs(seed: int = 0) -> dict:
    streams_of = jax.random.split(jax.random.key(seed), 12)
    saved_input = gaussian_with(streams_of[0], (TOKENS, D), 1.0, 24.0, ((0, 128),), (0, 1, 128, 5.5))
    cot_inproj = normal_values(streams_of[1], (TOKENS, GN), (TOKENS ** -0.5), 0.019042969, ((0, 128), (1, 4)))
    cot_outproj = normal_values(streams_of[2], (TOKENS, GN), (TOKENS ** -0.5), 0.019042969, ((0, 128), (1, 4)))
    factor_inproj = draw_factor_inproj(jax.random.fold_in(streams_of[11], 71), 0)
    factor_outproj = draw_factor_outproj(jax.random.fold_in(streams_of[11], 71), 0)
    weight_inproj = normal_values(streams_of[5], (D, GN), D ** -0.5, 0.125, ((0, 128), (1, 4)), jnp.float32)
    weight_outproj = normal_values(streams_of[6], (D, GN), D ** -0.5, 0.125, ((0, 128), (1, 4)), jnp.float32)
    first_inproj = normal_values(streams_of[7], (RANK, GN), 1.0, 6.0, ((0, 128), (1, 4)), jnp.float32)
    first_outproj = normal_values(streams_of[8], (RANK, GN), 1.0, 6.0, ((0, 128), (1, 4)), jnp.float32)
    second_inproj = jnp.clip(jnp.exp(math.log(4.0) - 2.7725887 * jax.random.uniform(streams_of[9], (RANK, GN), jnp.float32) ** levels(streams_of[9], (RANK, GN), ((0, 128), (1, 4)), -0.2, 0.2)), 0.25, 4.0)
    second_outproj = jnp.clip(jnp.exp(math.log(4.0) - 2.7725887 * jax.random.uniform(streams_of[10], (RANK, GN), jnp.float32) ** levels(streams_of[10], (RANK, GN), ((0, 128), (1, 4)), -0.2, 0.2)), 0.25, 4.0)
    return dict(saved_input=saved_input, cot_inproj=cot_inproj, cot_outproj=cot_outproj, factor_inproj=factor_inproj, factor_outproj=factor_outproj, weight_inproj=weight_inproj, weight_outproj=weight_outproj, first_inproj=first_inproj, first_outproj=first_outproj, second_inproj=second_inproj, second_outproj=second_outproj)


def one_matrix(saved_input, cotangent, factor, weight, first, second):
    grad = lax.dot_general(saved_input, cotangent, (((0,), (0,)), ((), ())), preferred_element_type=jnp.float32)
    factor_wide = factor.astype(jnp.float32)
    projected = lax.dot_general(factor_wide, grad, (((0,), (0,)), ((), ())), precision=lax.Precision.HIGHEST)
    first_new = 0.8 * first + 0.2 * projected
    second_new = 0.9 * second + 0.1 * projected * projected
    small = first_new / (jnp.sqrt(second_new) + 1e-08)
    full = jnp.dot(factor_wide, small, precision=lax.Precision.HIGHEST)
    update = full / jnp.sqrt(jnp.mean(full * full) + 1e-06)
    fresh = weight - 0.02 * update
    return (update, fresh, fresh.astype(jnp.bfloat16), first_new, second_new)

def reference(saved_input, cot_inproj, cot_outproj, factor_inproj, factor_outproj, weight_inproj, weight_outproj, first_inproj, first_outproj, second_inproj, second_outproj):
    in_parts = one_matrix(saved_input, cot_inproj, factor_inproj, weight_inproj, first_inproj, second_inproj)
    out_parts = one_matrix(saved_input, cot_outproj, factor_outproj, weight_outproj, first_outproj, second_outproj)
    return (in_parts[0], out_parts[0], in_parts[1], out_parts[1], in_parts[2], out_parts[2], in_parts[3], out_parts[3], in_parts[4], out_parts[4])
```

```python
import functools

import jax
import jax.numpy as jnp
from jax import lax
from jax.experimental import pallas as pl
from jax.experimental.pallas import tpu as pltpu
from jax.sharding import PartitionSpec as P

MESH = pl.DeviceIdType.MESH
F32 = jnp.float32
BF16 = jnp.bfloat16
FAR_FIRST = (4, 3, 5, 2, 6, 1, 7)
NEAR_FIRST = (1, 7, 2, 6, 3, 5, 4)
ROWS_FIRST = (((0,), (0,)), ((), ()))


def rank_order():
    r = lax.broadcasted_iota(jnp.int32, (256, 256), 0)
    p = lax.broadcasted_iota(jnp.int32, (256, 256), 1)
    target = ((r >> 2) & 7) * 32 + (r >> 5) * 4 + (r & 3)
    return jnp.where(target == p, 1.0, 0.0).astype(BF16)


def halves(value):
    high = value.astype(BF16)
    return high, (value - high.astype(F32)).astype(BF16)


def kernel(
    entries,
    saved, cot_in, cot_out, f_in, f_out, w_in, w_out, m1_in, m1_out, m2_in, m2_out,
    upd_in, upd_out, new_in, new_out, copies, fst_in, fst_out, snd_in, snd_out,
    s_v, c_v, fl, ft, wl, r1_in, r1_out, r2_in, r2_out, mo, mg, m1c, m2c,
    fg, gh, gl, pp, prx, ps, rb, ab, sm, full, wg, qb, stage, arrived, nst, nrx,
    load_sem, a1_send, a1_recv, mo_send, mo_recv, w1_send, w1_recv, w2_send, w2_recv,
    a2_send, a2_recv, part_send, part_recv, b1_send, b1_recv, b2_send, b2_recv,
    b3_send, b3_recv, c_send, c_recv, q_send, q_recv, n_send, n_recv, o_send, o_recv,
    e_send, e_recv,
):
    me, x = lax.axis_index("fs"), lax.axis_index("tp")
    c = lax.rem(me, 2)
    y = lax.rem(lax.div(me, 2), 8)
    z = lax.div(me, 16)
    u = z + c * (y - z)
    v = y + c * (z - y)
    other = 1 - c

    def plus(at, k):
        return lax.rem(at + k % 8, 8)

    def dev(zz, yy, cc):
        return ((zz * 8 + yy) * 2 + cc, x)

    def along_u(k):
        to = plus(u, k)
        return dev(to + c * (v - to), v + c * (to - v), c)

    def along_v(k):
        to = plus(v, k)
        return dev(u + c * (to - u), to + c * (u - to), c)

    partner = dev(z, y, other)
    sent = []

    def send(src, dst, send_sem, recv_sem, device):
        copy = pltpu.make_async_remote_copy(
            src_ref=src, dst_ref=dst, send_sem=send_sem, recv_sem=recv_sem,
            device_id=device, device_id_type=MESH,
        )
        copy.start()
        sent.append(copy)

    def arrive(dst, recv_sem):
        pltpu.make_async_copy(dst, dst, recv_sem).wait()

    loads = {}

    def load(name, src, dst):
        loads[name] = pltpu.make_async_copy(src, dst, load_sem.at[len(loads)])
        loads[name].start()

    load("f_in", f_in, fl.at[0])
    load("f_out", f_out, ft)
    load("m1_in", m1_in, r1_in)
    load("m1_out", m1_out, r1_out)
    load("m2_in", m2_in, r2_in)
    load("m2_out", m2_out, r2_out)
    load("w_in", w_in, wl.at[0])
    load("w_out", w_out, wl.at[1])
    load("c_in", cot_in, c_v.at[:, 0:256])
    load("c_out", cot_out, c_v.at[:, 256:512])
    load("saved", saved, s_v)

    barrier = pltpu.get_barrier_semaphore()
    peers = [partner]
    for k in range(1, 8):
        for cc in range(2):
            peers.append(dev(plus(z, k), y, cc))
            peers.append(dev(z, plus(y, k), cc))
    for k in range(1, 4):
        peers.append((me, lax.rem(x + k, 4)))
    for peer in peers:
        pl.semaphore_signal(barrier, inc=1, device_id=peer, device_id_type=MESH)

    order = rank_order()
    for name in ("f_in", "f_out", "m1_in", "m1_out", "m2_in", "m2_out"):
        loads[name].wait()
    fl[1] = jnp.dot(ft[...], order, preferred_element_type=F32).astype(BF16)
    fg[c, v, u, c] = fl[c]
    mo[0, 0:2] = r1_in[...]
    mo[0, 2:4] = r2_in[...]
    mo[1, 0:2] = r1_out[...]
    mo[1, 2:4] = r2_out[...]
    mg[v, c] = mo[c]
    loads["w_in"].wait()
    loads["w_out"].wait()
    wg[v, u, c] = wl[c]
    pl.semaphore_wait(barrier, len(peers))

    def to_line(X, k):
        return dev(plus(z, k), y, 0) if X == 0 else dev(z, plus(y, k), 1)

    def to_cross(X, k):
        return dev(z, plus(y, k), 0) if X == 0 else dev(plus(z, k), y, 1)

    at_u, at_v = (z, y), (y, z)
    for k in FAR_FIRST:
        for X in range(2):
            send(fl.at[X], fg.at[X, at_v[X], at_u[X], c], a1_send.at[X, k], a1_recv.at[k, c], to_line(X, k))
    send(fl.at[other], fg.at[other, u, v, c], a1_send.at[0, 0], a1_recv.at[0, c], partner)
    for k in FAR_FIRST:
        for X in range(2):
            send(mo.at[X], mg.at[at_v[X], c], mo_send.at[X, k], mo_recv.at[k, c], to_cross(X, k))
    send(mo.at[other], mg.at[u, c], mo_send.at[0, 0], mo_recv.at[0, c], partner)
    for k in FAR_FIRST:
        for X in range(2):
            send(wl.at[X], wg.at[at_v[X], at_u[X], c], w1_send.at[X, k], w1_recv.at[k, c], to_line(X, k))
    send(wl.at[other], wg.at[u, v, c], w1_send.at[0, 0], w1_recv.at[0, c], partner)

    loads["c_in"].wait()
    loads["c_out"].wait()
    loads["saved"].wait()

    def grad(zc, carry):
        at = pl.ds(pl.multiple_of(zc * 256, 256), 256)
        g = lax.dot_general(s_v[:, at], c_v[...], ROWS_FIRST, preferred_element_type=F32)
        high, low = halves(g)
        high, low = high.reshape(8, 32, 512), low.reshape(8, 32, 512)
        gh[0, :, zc] = high[:, :, 0:256]
        gl[0, :, zc] = low[:, :, 0:256]
        gh[1, zc] = high[:, :, 256:512]
        gl[1, zc] = low[:, :, 256:512]
        return carry

    lax.fori_loop(0, 4, grad, 0)

    for k in NEAR_FIRST:
        for cc in range(2):
            arrive(fg.at[c, v, plus(u, -k), cc], a1_recv.at[k, cc])
    arrive(fg.at[c, v, u, other], a1_recv.at[0, other])

    def pass_on(j, part_k):
        at = fg.at[c, plus(v, j)]
        send(at, at, part_send.at[part_k], part_recv.at[part_k], partner)

    line = fg.at[c, v]
    for i, k in enumerate((2, -2, 1, -1)):
        send(line, line, a2_send.at[i], a2_recv.at[i], along_v(k))
    pass_on(0, 0)

    lax.fori_loop(4, 8, grad, 0)

    def project(X, j):
        f = fg[X, j].reshape(256, 256)
        term = lax.dot_general(f, gh[X, j].reshape(256, 256), ROWS_FIRST, preferred_element_type=F32)
        term += lax.dot_general(f, gl[X, j].reshape(256, 256), ROWS_FIRST, preferred_element_type=F32)
        return term.reshape(8, 32, 256)

    low, high = pl.ds(0, 4), pl.ds(4, 4)
    left, right = fg.at[c, plus(v, -2)], fg.at[c, plus(v, 2)]
    arrive(left, a2_recv.at[0])
    send(left, left, a2_send.at[4], a2_recv.at[4], along_v(1))
    send(left.at[low], left.at[low], a2_send.at[6], a2_recv.at[6], along_v(2))
    arrive(right, a2_recv.at[1])
    send(right, right, a2_send.at[5], a2_recv.at[5], along_v(-1))
    send(right.at[high], right.at[high], a2_send.at[7], a2_recv.at[7], along_v(-2))
    pass_on(-2, 1)
    pass_on(2, 2)
    arrive(fg.at[c, plus(v, -1)], a2_recv.at[2])
    pass_on(-1, 3)
    arrive(fg.at[c, plus(v, 1)], a2_recv.at[3])
    pass_on(1, 4)

    for k in NEAR_FIRST:
        for cc in range(2):
            arrive(wg.at[v, plus(u, -k), cc], w1_recv.at[k, cc])
    arrive(wg.at[v, u, other], w1_recv.at[0, other])

    def weight_step(s):
        a, b = plus(v, 1 - s), plus(v, s - 1)
        if s > 1:
            arrive(wg.at[a], w2_recv.at[0, s - 1])
            arrive(wg.at[b], w2_recv.at[1, s - 1])
        up, down = wg.at[a], wg.at[b]
        if s == 4:
            up, down = up.at[low], down.at[high]
        send(up, up, w2_send.at[0, s], w2_recv.at[0, s], along_v(1))
        send(down, down, w2_send.at[1, s], w2_recv.at[1, s], along_v(-1))

    weight_step(1)

    for k in NEAR_FIRST:
        for cc in range(2):
            arrive(mg.at[plus(v, -k), cc], mo_recv.at[k, cc])
    arrive(mg.at[v, other], mo_recv.at[0, other])
    for k in range(8):
        for cc in range(2):
            at = 4 * k + 2 * cc
            m1c[at:at + 2] = mg[k, cc, 0:2]
            m2c[at:at + 2] = mg[k, cc, 2:4]

    pp[c] = project(c, v)
    arrive(fg.at[other, u], part_recv.at[0])
    pp[other] = project(other, u)
    for j, part_k in ((-2, 1), (2, 2), (-1, 3), (1, 4)):
        pp[c] += project(c, plus(v, j))
        arrive(fg.at[other, plus(u, j)], part_recv.at[part_k])
        pp[other] += project(other, plus(u, j))
    arrive(fg.at[c, plus(v, -3)], a2_recv.at[4])
    pass_on(-3, 5)
    arrive(fg.at[c, plus(v, 3)], a2_recv.at[5])
    pass_on(3, 6)
    pp[c] += project(c, plus(v, -3))
    pp[c] += project(c, plus(v, 3))
    arrive(fg.at[c, plus(v, 4), low], a2_recv.at[6])
    arrive(fg.at[c, plus(v, 4), high], a2_recv.at[7])
    pass_on(4, 7)
    for j, part_k in ((-3, 5), (3, 6), (4, 7)):
        arrive(fg.at[other, plus(u, j)], part_recv.at[part_k])
        pp[other] += project(other, plus(u, j))

    for k in FAR_FIRST + (0,):
        at = plus(v, k)
        send(pp.at[other, at], prx.at[at], b1_send.at[k], b1_recv.at[k], partner)
    pp[c] += project(c, plus(v, 4))
    for k in FAR_FIRST + (0,):
        at = plus(u, k)
        arrive(prx.at[at], b1_recv.at[k])
        ps[at] = pp[c, at] + prx[at]
        if k:
            send(ps.at[at], rb.at[u], b2_send.at[k], b2_recv.at[k], along_u(k))
    weight_step(2)
    total = ps[u]
    for k in NEAR_FIRST:
        at = plus(u, -k)
        arrive(rb.at[at], b2_recv.at[k])
        total += rb[at]
    ab[v] = total

    for k in FAR_FIRST:
        send(ab.at[v], ab.at[v], b3_send.at[k], b3_recv.at[k], along_v(k))
    weight_step(3)
    for k in NEAR_FIRST:
        arrive(ab.at[plus(v, -k)], b3_recv.at[k])
    projected = ab[0]
    for k in range(1, 8):
        projected += ab[k]
    first = 0.8 * m1c[...] + 0.2 * projected
    second = 0.9 * m2c[...] + 0.1 * projected * projected
    sm[u] = first / (jnp.sqrt(second) + 1e-08)
    for k in FAR_FIRST:
        send(sm.at[u], sm.at[u], c_send.at[k], c_recv.at[k], along_u(k))
    weight_step(4)
    m1c[...] = first
    m2c[...] = second
    theirs = 4 * v + 2 * other
    for i in range(2):
        nst[i:i + 1] = m1c[pl.ds(theirs + i, 1)]
        nst[2 + i:3 + i] = m2c[pl.ds(theirs + i, 1)]
    send(nst, nrx, n_send, n_recv, partner)
    for k in NEAR_FIRST:
        arrive(sm.at[plus(u, -k)], c_recv.at[k])

    small_high, small_low = halves(sm[...].reshape(256, 256))

    def expand(j, squares):
        f = fg[c, j].reshape(256, 256)
        value = jnp.dot(f, small_high, preferred_element_type=F32)
        value += jnp.dot(f, small_low, preferred_element_type=F32)
        full[j] = value.reshape(8, 2, 16, 256)
        return squares + jnp.sum((value * value).reshape(32, 8, 256), axis=0)

    squares = lax.fori_loop(0, 8, expand, jnp.zeros((8, 256), F32))
    qb[x] = jnp.broadcast_to(jnp.sum(squares, keepdims=True), (8, 128))
    for k in (2, 1, 3):
        send(qb.at[x], qb.at[x], q_send.at[k], q_recv.at[k], (me, lax.rem(x + k, 4)))
    arrive(wg.at[plus(v, 4), low], w2_recv.at[0, 4])
    arrive(wg.at[plus(v, 4), high], w2_recv.at[1, 4])
    for k in (1, 3, 2):
        arrive(qb.at[lax.rem(x + 4 - k, 4)], q_recv.at[k])
    square = ((qb[0] + qb[1]) + qb[2]) + qb[3]
    scale = 1.0 / jnp.sqrt(square[0:1] / entries + 1e-06)
    scale = jnp.concatenate([scale, scale], axis=1)

    their_update = full[v, u, other] * scale
    stage[0] = their_update
    stage[1] = wg[v, u, other] - 0.02 * their_update
    send(stage, arrived, o_send, o_recv, partner)
    for j in range(8):
        update = full[j].reshape(256, 256) * scale
        fresh = wg[j].reshape(256, 256) - 0.02 * update
        copies[c, j] = fresh.astype(BF16).reshape(8, 32, 256)
        send(copies.at[c, j], copies.at[c, j], e_send.at[j], e_recv.at[j], partner)
    my_update = full[v, u, c] * scale
    my_new = wg[v, u, c] - 0.02 * my_update
    is_in = c == 0
    mine = 4 * v + 2 * c
    my_first = jnp.concatenate([m1c[pl.ds(mine, 1)], m1c[pl.ds(mine + 1, 1)]], axis=0)
    my_second = jnp.concatenate([m2c[pl.ds(mine, 1)], m2c[pl.ds(mine + 1, 1)]], axis=0)
    arrive(nrx, n_recv)
    fst_in[...] = jnp.where(is_in, my_first, nrx[0:2])
    fst_out[...] = jnp.where(is_in, nrx[0:2], my_first)
    snd_in[...] = jnp.where(is_in, my_second, nrx[2:4])
    snd_out[...] = jnp.where(is_in, nrx[2:4], my_second)
    arrive(arrived, o_recv)
    upd_in[...] = jnp.where(is_in, my_update, arrived[0])
    upd_out[...] = jnp.where(is_in, arrived[0], my_update)
    new_in[...] = jnp.where(is_in, my_new, arrived[1])
    new_out[...] = jnp.where(is_in, arrived[1], my_new)
    for j in range(8):
        arrive(copies.at[other, j], e_recv.at[j])
    for copy in sent:
        copy.wait_send()


def on_device(*args):
    shape = jax.ShapeDtypeStruct
    rows = shape((16, 256), F32)
    pair = shape((2, 256), F32)
    dma = pltpu.SemaphoreType.DMA
    vmem = pltpu.VMEM
    scratch = [
        vmem((768, 2048), BF16), vmem((768, 512), BF16),
        vmem((2, 16, 256), BF16), vmem((16, 256), BF16), vmem((2, 16, 256), F32),
        vmem((2, 256), F32), vmem((2, 256), F32), vmem((2, 256), F32), vmem((2, 256), F32),
        vmem((2, 8, 256), F32), vmem((8, 2, 8, 256), F32),
        vmem((32, 256), F32), vmem((32, 256), F32),
        vmem((2, 8, 8, 2, 16, 256), BF16),
        vmem((2, 8, 8, 32, 256), BF16), vmem((2, 8, 8, 32, 256), BF16),
        vmem((2, 8, 32, 256), F32), vmem((8, 32, 256), F32), vmem((8, 32, 256), F32),
        vmem((8, 32, 256), F32), vmem((8, 32, 256), F32), vmem((8, 32, 256), F32),
        vmem((8, 8, 2, 16, 256), F32), vmem((8, 8, 2, 16, 256), F32),
        vmem((4, 8, 128), F32), vmem((2, 16, 256), F32), vmem((2, 16, 256), F32),
        vmem((8, 256), F32), vmem((8, 256), F32),
        dma((11,)),
        dma((2, 8)), dma((8, 2)), dma((2, 8)), dma((8, 2)), dma((2, 8)), dma((8, 2)),
        dma((2, 5)), dma((2, 5)),
        dma((8,)), dma((8,)), dma((8,)), dma((8,)), dma((8,)), dma((8,)),
        dma((8,)), dma((8,)), dma((8,)), dma((8,)), dma((8,)), dma((8,)),
        dma((4,)), dma((4,)), dma, dma, dma, dma, dma((8,)), dma((8,)),
    ]
    scratch = [s(()) if s is dma else s for s in scratch]
    upd_in, upd_out, new_in, new_out, copies, fst_in, fst_out, snd_in, snd_out = pl.pallas_call(
        functools.partial(kernel, float(2048 * 1024)),
        out_shape=(rows, rows, rows, rows, shape((2, 8, 8, 32, 256), BF16), pair, pair, pair, pair),
        in_specs=[pl.BlockSpec(memory_space=pl.ANY)] * 11,
        out_specs=(pl.BlockSpec(memory_space=pltpu.VMEM),) * 9,
        scratch_shapes=scratch,
        compiler_params=pltpu.CompilerParams(collective_id=0, has_side_effects=True),
    )(*args)
    copy_in = jnp.swapaxes(copies[0], 0, 1).reshape(2048, 256)
    copy_out = copies[1].reshape(2048, 256)
    return (upd_in, upd_out, new_in, new_out, copy_in, copy_out, fst_in, fst_out, snd_in, snd_out)


def solution(mesh):
    both, rows, columns = P("fs", "tp"), P("fs", None), P(None, "tp")
    return jax.shard_map(
        on_device,
        mesh=mesh,
        in_specs=(rows, both, both, rows, rows) + (both,) * 6,
        out_specs=(both,) * 4 + (columns,) * 2 + (both,) * 4,
        check_vma=False,
    )
```

```python
import functools

import jax
import jax.numpy as jnp
from jax import lax
from jax.experimental import pallas as pl
from jax.experimental.pallas import tpu as pltpu
from jax.sharding import PartitionSpec as P

MESH = pl.DeviceIdType.MESH
F32 = jnp.float32
BF16 = jnp.bfloat16
FAR_FIRST = (4, 3, 5, 2, 6, 1, 7)
NEAR_FIRST = (1, 7, 2, 6, 3, 5, 4)
ROWS_FIRST = (((0,), (0,)), ((), ()))


def rank_order():
    r = lax.broadcasted_iota(jnp.int32, (256, 256), 0)
    p = lax.broadcasted_iota(jnp.int32, (256, 256), 1)
    target = ((r >> 2) & 7) * 32 + (r >> 5) * 4 + (r & 3)
    return jnp.where(target == p, 1.0, 0.0).astype(BF16)


def halves(value):
    high = value.astype(BF16)
    return high, (value - high.astype(F32)).astype(BF16)


def kernel(
    entries,
    saved, cot_in, cot_out, f_in, f_out, w_in, w_out, m1_in, m1_out, m2_in, m2_out,
    copies, rows, moments,
    s_v, c_v, fl, ft, wl, r1_in, r1_out, r2_in, r2_out, mo, mg, m1c, m2c,
    fg, go, gs, gr, gh, gl, pp, rb, ab, sm, full, wg, qb, nst, nrx,
    load_sem, a1_send, a1_recv, mo_send, mo_recv, w1_send, w1_recv, w2_send, w2_recv,
    near_send, near_recv, two_recv, three_send, three_recv, four_send, four_recv,
    fp_send, fp_recv, wp_send, wp_recv, g_send, g_recv, b2_send, b2_recv,
    b3_send, b3_recv, c_send, c_recv, sp_send, sp_recv, q_send, q_recv, n_send, n_recv,
):
    me, x = lax.axis_index("fs"), lax.axis_index("tp")
    c = lax.rem(me, 2)
    y = lax.rem(lax.div(me, 2), 8)
    z = lax.div(me, 16)
    u = z + c * (y - z)
    v = y + c * (z - y)
    other = 1 - c

    def plus(at, k):
        return lax.rem(at + k % 8, 8)

    def dev(zz, yy, cc):
        return ((zz * 8 + yy) * 2 + cc, x)

    def along_u(k):
        to = plus(u, k)
        return dev(to + c * (v - to), v + c * (to - v), c)

    def along_v(k):
        to = plus(v, k)
        return dev(u + c * (to - u), to + c * (u - to), c)

    partner = dev(z, y, other)
    sent = []

    def send(src, dst, send_sem, recv_sem, device, later=True):
        copy = pltpu.make_async_remote_copy(
            src_ref=src, dst_ref=dst, send_sem=send_sem, recv_sem=recv_sem,
            device_id=device, device_id_type=MESH,
        )
        copy.start()
        if later:
            sent.append(copy)

    def arrive(dst, sem):
        pltpu.make_async_copy(dst, dst, sem).wait()

    loads = {}

    def load(name, src, dst):
        loads[name] = pltpu.make_async_copy(src, dst, load_sem.at[len(loads)])
        loads[name].start()

    load("f_in", f_in, fl.at[0])
    load("f_out", f_out, ft)
    load("m1_in", m1_in, r1_in)
    load("m1_out", m1_out, r1_out)
    load("m2_in", m2_in, r2_in)
    load("m2_out", m2_out, r2_out)
    load("w_in", w_in, wl.at[0])
    load("w_out", w_out, wl.at[1])
    load("c_in", cot_in, c_v.at[:, pl.ds(pl.multiple_of(256 * c, 256), 256)])
    load("c_out", cot_out, c_v.at[:, pl.ds(pl.multiple_of(256 * other, 256), 256)])
    load("saved", saved, s_v)

    barrier = pltpu.get_barrier_semaphore()
    peers = [partner]
    for k in range(1, 8):
        for cc in range(2):
            peers.append(dev(plus(z, k), y, cc))
            peers.append(dev(z, plus(y, k), cc))
    for k in range(1, 4):
        peers.append((me, lax.rem(x + k, 4)))
        peers.append((me + 1 - 2 * c, lax.rem(x + k, 4)))
    for peer in peers:
        pl.semaphore_signal(barrier, inc=1, device_id=peer, device_id_type=MESH)

    order = rank_order()
    for name in ("f_in", "f_out", "m1_in", "m1_out", "m2_in", "m2_out"):
        loads[name].wait()
    fl[1] = jnp.dot(ft[...], order, preferred_element_type=F32).astype(BF16)
    fg[c, v, u, c] = fl[c]
    mo[0, 0:2] = r1_in[...]
    mo[0, 2:4] = r2_in[...]
    mo[1, 0:2] = r1_out[...]
    mo[1, 2:4] = r2_out[...]
    mg[v, c] = mo[c]
    loads["w_in"].wait()
    loads["w_out"].wait()
    wg[c, v, u, c] = wl[c]
    pl.semaphore_wait(barrier, len(peers))

    def to_line(X, k):
        return dev(plus(z, k), y, 0) if X == 0 else dev(z, plus(y, k), 1)

    def to_cross(X, k):
        return dev(z, plus(y, k), 0) if X == 0 else dev(plus(z, k), y, 1)

    at_u, at_v = (z, y), (y, z)
    send(fl.at[other], fg.at[other, u, v, c], a1_send.at[0, 0], a1_recv.at[0, c], partner)
    for k in FAR_FIRST:
        for X in range(2):
            send(fl.at[X], fg.at[X, at_v[X], at_u[X], c], a1_send.at[X, k], a1_recv.at[k, c], to_line(X, k))

    def spread(k):
        block = fg.at[c, v, plus(u, -k)]
        if k:
            arrive(fg.at[c, v, plus(u, -k), 0], a1_recv.at[k, 0])
            arrive(fg.at[c, v, plus(u, -k), 1], a1_recv.at[k, 1])
        else:
            arrive(fg.at[c, v, u, other], a1_recv.at[0, other])
        send(block, block, near_send.at[0], two_recv.at[0, k], along_v(2), later=False)
        send(block, block, near_send.at[1], two_recv.at[1, k], along_v(-2), later=False)
        send(block, block, near_send.at[2], near_recv.at[0], along_v(1), later=False)
        send(block, block, near_send.at[3], near_recv.at[1], along_v(-1), later=False)

    spread(0)
    for k in FAR_FIRST:
        for X in range(2):
            send(wl.at[X], wg.at[X, at_v[X], at_u[X], c], w1_send.at[X, k], w1_recv.at[k, c], to_line(X, k))
    send(wl.at[other], wg.at[other, u, v, c], w1_send.at[0, 0], w1_recv.at[0, c], partner)

    loads["c_in"].wait()
    loads["c_out"].wait()
    loads["saved"].wait()

    def grad_copy(zc):
        return pltpu.make_async_remote_copy(
            src_ref=gs.at[zc], dst_ref=gr.at[zc], send_sem=g_send.at[zc], recv_sem=g_recv.at[zc],
            device_id=partner, device_id_type=MESH,
        )

    def grad(zc, carry):
        at = pl.ds(pl.multiple_of(zc * 256, 256), 256)
        g = lax.dot_general(s_v[:, at], c_v[...], ROWS_FIRST, preferred_element_type=F32)
        gs[zc] = g[:, 256:512]
        go[zc] = g[:, 0:256]
        grad_copy(zc).start()
        return carry

    lax.fori_loop(0, 4, grad, 0)

    for k in NEAR_FIRST:
        spread(k)

    for k in FAR_FIRST:
        for X in range(2):
            send(mo.at[X], mg.at[at_v[X], c], mo_send.at[X, k], mo_recv.at[k, c], to_cross(X, k))
    send(mo.at[other], mg.at[u, c], mo_send.at[0, 0], mo_recv.at[0, c], partner)
    lax.fori_loop(4, 8, grad, 0)

    for i, k in enumerate((0,) + NEAR_FIRST):
        left, right = fg.at[c, plus(v, -2), plus(u, -k)], fg.at[c, plus(v, 2), plus(u, -k)]
        arrive(left, two_recv.at[0, k])
        send(left, left, three_send.at[0], three_recv.at[0], along_v(1), later=False)
        if i % 2:
            send(left, left, four_send.at[k], four_recv.at[k], along_v(2))
        arrive(right, two_recv.at[1, k])
        send(right, right, three_send.at[1], three_recv.at[1], along_v(-1), later=False)
        if i % 2 == 0:
            send(right, right, four_send.at[k], four_recv.at[k], along_v(-2))
    half = (pl.ds(0, 4), pl.ds(4, 4))

    def pass_weight(j, i):
        at = wg.at[c, plus(v, j)]
        send(at, at, wp_send.at[i], wp_recv.at[i], partner)

    def weight_step(s):
        a, b = plus(v, 1 - s), plus(v, s - 1)
        up, down = wg.at[c, a], wg.at[c, b]
        if s > 1:
            arrive(up, w2_recv.at[0, s - 1])
            arrive(down, w2_recv.at[1, s - 1])
        if s == 4:
            up, down = up.at[half[0]], down.at[half[1]]
        send(up, up, w2_send.at[0, s], w2_recv.at[0, s], along_v(1))
        send(down, down, w2_send.at[1, s], w2_recv.at[1, s], along_v(-1))
        if s == 1:
            pass_weight(0, 0)
        else:
            pass_weight(1 - s, 2 * s - 3)
            pass_weight(s - 1, 2 * s - 2)

    for k in NEAR_FIRST:
        for cc in range(2):
            arrive(wg.at[c, v, plus(u, -k), cc], w1_recv.at[k, cc])
    arrive(wg.at[c, v, u, other], w1_recv.at[0, other])
    weight_step(1)
    def combine(zc, carry):
        pltpu.make_async_copy(gr.at[zc], gr.at[zc], g_recv.at[zc]).wait()
        high, low = halves(go[zc] + gr[zc])
        for i in range(8):
            a, b = i + c * (zc - i), zc + c * (i - zc)
            gh[a, b] = high[32 * i:32 * i + 32]
            gl[a, b] = low[32 * i:32 * i + 32]
        return carry

    lax.fori_loop(0, 8, combine, 0)

    def project(j):
        f = fg[c, j].reshape(256, 256)
        term = lax.dot_general(f, gh[j].reshape(256, 256), ROWS_FIRST, preferred_element_type=F32)
        term += lax.dot_general(f, gl[j].reshape(256, 256), ROWS_FIRST, preferred_element_type=F32)
        return term.reshape(8, 32, 256)

    def pass_factor(j, i):
        at = fg.at[c, plus(v, j)]
        send(at, at, fp_send.at[i], fp_recv.at[i], partner)

    pass_factor(0, 0)
    pass_factor(-2, 1)
    pass_factor(2, 2)
    pp[...] = project(v)
    pp[...] += project(plus(v, -2))
    pp[...] += project(plus(v, 2))
    arrive(fg.at[c, plus(v, -1)], near_recv.at[0])
    pp[...] += project(plus(v, -1))
    arrive(fg.at[c, plus(v, 1)], near_recv.at[1])
    pp[...] += project(plus(v, 1))
    pass_factor(-1, 3)
    pass_factor(1, 4)
    arrive(fg.at[c, plus(v, -3)], three_recv.at[0])
    pp[...] += project(plus(v, -3))
    arrive(fg.at[c, plus(v, 3)], three_recv.at[1])
    pp[...] += project(plus(v, 3))
    for k in (0,) + NEAR_FIRST:
        arrive(fg.at[c, plus(v, 4), plus(u, -k)], four_recv.at[k])
    pp[...] += project(plus(v, 4))
    for k in FAR_FIRST:
        send(pp.at[plus(u, k)], rb.at[u], b2_send.at[k], b2_recv.at[k], along_u(k))
    pass_factor(-3, 5)
    pass_factor(3, 6)
    pass_factor(4, 7)

    for k in NEAR_FIRST:
        for cc in range(2):
            arrive(mg.at[plus(v, -k), cc], mo_recv.at[k, cc])
    arrive(mg.at[v, other], mo_recv.at[0, other])
    for k in range(8):
        for cc in range(2):
            at = 4 * k + 2 * cc
            m1c[at:at + 2] = mg[k, cc, 0:2]
            m2c[at:at + 2] = mg[k, cc, 2:4]

    weight_step(2)
    total = pp[u]
    for k in NEAR_FIRST:
        at = plus(u, -k)
        arrive(rb.at[at], b2_recv.at[k])
        total += rb[at]
    ab[v] = total

    for k in FAR_FIRST:
        send(ab.at[v], ab.at[v], b3_send.at[k], b3_recv.at[k], along_v(k))
    weight_step(3)
    for k in NEAR_FIRST:
        arrive(ab.at[plus(v, -k)], b3_recv.at[k])
    projected = ab[0]
    for k in range(1, 8):
        projected += ab[k]
    first = 0.8 * m1c[...] + 0.2 * projected
    second = 0.9 * m2c[...] + 0.1 * projected * projected
    sm[c, u] = first / (jnp.sqrt(second) + 1e-08)
    for k in FAR_FIRST:
        send(sm.at[c, u], sm.at[c, u], c_send.at[k], c_recv.at[k], along_u(k))
    send(sm.at[c, u], sm.at[c, u], sp_send.at[0], sp_recv.at[0], partner)
    m1c[...] = first
    m2c[...] = second
    theirs = 4 * v + 2 * other
    for i in range(2):
        nst[i:i + 1] = m1c[pl.ds(theirs + i, 1)]
        nst[2 + i:3 + i] = m2c[pl.ds(theirs + i, 1)]
    send(nst, nrx, n_send, n_recv, partner)
    weight_step(4)
    for k in NEAR_FIRST:
        at = sm.at[c, plus(u, -k)]
        arrive(at, c_recv.at[k])
        send(at, at, sp_send.at[k], sp_recv.at[k], partner)

    def expanded(X):
        high, low = halves(sm[X].reshape(256, 256))
        small = jnp.concatenate([high, low], axis=0)

        def expand(j, squares):
            f = fg[X, j].reshape(256, 256)
            value = jnp.dot(jnp.concatenate([f, f], axis=1), small, preferred_element_type=F32)
            full[X, j] = value.reshape(8, 2, 16, 256)
            return squares + jnp.sum((value * value).reshape(32, 8, 256), axis=0)

        return lax.fori_loop(0, 8, expand, jnp.zeros((8, 256), F32), unroll=2)

    squares = expanded(c)
    qb[c, x] = jnp.broadcast_to(jnp.sum(squares, keepdims=True), (8, 128))
    mine = qb.at[c, x]
    for k in (2, 1, 3):
        to = lax.rem(x + k, 4)
        send(mine, mine, q_send.at[k, 0], q_recv.at[k, 0], (me, to))
        send(mine, mine, q_send.at[k, 1], q_recv.at[k, 1], (me + 1 - 2 * c, to))
    send(mine, mine, q_send.at[0, 1], q_recv.at[0, 1], partner)
    four = wg.at[c, plus(v, 4)]
    arrive(four.at[half[0]], w2_recv.at[0, 4])
    arrive(four.at[half[1]], w2_recv.at[1, 4])
    pass_weight(4, 7)
    for j, i in ((0, 0), (-2, 1), (2, 2), (-1, 3), (1, 4), (-3, 5), (3, 6), (4, 7)):
        arrive(fg.at[other, plus(u, j)], fp_recv.at[i])
    for k in (0,) + NEAR_FIRST:
        arrive(sm.at[other, plus(v, -k)], sp_recv.at[k])
    expanded(other)
    for k in (1, 3, 2):
        arrive(qb.at[c, lax.rem(x + 4 - k, 4)], q_recv.at[k, 0])
        arrive(qb.at[other, lax.rem(x + 4 - k, 4)], q_recv.at[k, 1])
    arrive(qb.at[other, x], q_recv.at[0, 1])

    def scale_of(X):
        square = ((qb[X, 0] + qb[X, 1]) + qb[X, 2]) + qb[X, 3]
        scale = 1.0 / jnp.sqrt(square[0:1] / entries + 1e-06)
        return jnp.concatenate([scale, scale], axis=1)

    def finish(X, first_line, last_line):
        scale = scale_of(X)

        def line(j, carry):
            update = full[X, j].reshape(256, 256) * scale
            fresh = wg[X, j].reshape(256, 256) - 0.02 * update
            rounded = fresh.astype(BF16)
            for i in range(8):
                copies[X, i + X * (j - i), j + X * (i - j)] = rounded[32 * i:32 * i + 32]
            return carry

        lax.fori_loop(first_line, last_line, line, 0)

    finish(c, 0, 8)
    for X in range(2):
        update = full[X, at_v[X], at_u[X], c] * scale_of(X)
        rows[X] = update
        rows[2 + X] = wl[X] - 0.02 * update
    own = 4 * v + 2 * c
    my_first = jnp.concatenate([m1c[pl.ds(own, 1)], m1c[pl.ds(own + 1, 1)]], axis=0)
    my_second = jnp.concatenate([m2c[pl.ds(own, 1)], m2c[pl.ds(own + 1, 1)]], axis=0)
    arrive(nrx, n_recv)
    is_in = c == 0
    moments[0] = jnp.where(is_in, my_first, nrx[0:2])
    moments[1] = jnp.where(is_in, nrx[0:2], my_first)
    moments[2] = jnp.where(is_in, my_second, nrx[2:4])
    moments[3] = jnp.where(is_in, nrx[2:4], my_second)
    for j, i in ((0, 0), (-1, 1), (1, 2), (-2, 3), (2, 4), (-3, 5), (3, 6), (4, 7)):
        arrive(wg.at[other, plus(u, j)], wp_recv.at[i])
    finish(other, 0, 8)
    for copy in sent:
        copy.wait_send()
    for i in range(4):
        arrive(fg.at[c, v], near_send.at[i])
    arrive(fg.at[c, v], three_send.at[0])
    arrive(fg.at[c, v], three_send.at[1])

    def drained(zc, carry):
        grad_copy(zc).wait_send()
        return carry

    lax.fori_loop(0, 8, drained, 0)


def write_out(copies, rows, moments, *refs):
    outs, sems = refs[:-1], refs[-1]
    sources = [copies.at[0], copies.at[1]] + [rows.at[i] for i in range(4)] + [moments.at[i] for i in range(4)]
    writes = [pltpu.make_async_copy(src, dst, sems.at[i]) for i, (src, dst) in enumerate(zip(sources, outs))]
    for write in writes:
        write.start()
    for write in writes:
        write.wait()


def on_device(*args):
    shape = jax.ShapeDtypeStruct
    dma = pltpu.SemaphoreType.DMA
    vmem = pltpu.VMEM
    anywhere = pl.BlockSpec(memory_space=pl.ANY)
    scratch = [
        vmem((768, 2048), BF16), vmem((768, 512), BF16),
        vmem((2, 16, 256), BF16), vmem((16, 256), BF16), vmem((2, 16, 256), F32),
        vmem((2, 256), F32), vmem((2, 256), F32), vmem((2, 256), F32), vmem((2, 256), F32),
        vmem((2, 8, 256), F32), vmem((8, 2, 8, 256), F32),
        vmem((32, 256), F32), vmem((32, 256), F32),
        vmem((2, 8, 8, 2, 16, 256), BF16),
        vmem((8, 256, 256), F32), vmem((8, 256, 256), F32), vmem((8, 256, 256), F32),
        vmem((8, 8, 32, 256), BF16), vmem((8, 8, 32, 256), BF16),
        vmem((8, 32, 256), F32), vmem((8, 32, 256), F32),
        vmem((8, 32, 256), F32), vmem((2, 8, 32, 256), F32),
        vmem((2, 8, 8, 2, 16, 256), F32), vmem((2, 8, 8, 2, 16, 256), F32),
        vmem((2, 4, 8, 128), F32), vmem((8, 256), F32), vmem((8, 256), F32),
        dma((11,)),
        dma((2, 8)), dma((8, 2)), dma((2, 8)), dma((8, 2)), dma((2, 8)), dma((8, 2)),
        dma((2, 5)), dma((2, 5)),
        dma((4,)), dma((2,)), dma((2, 8)), dma((2,)), dma((2,)), dma((8,)), dma((8,)),
        dma((8,)), dma((8,)), dma((8,)), dma((8,)), dma((8,)), dma((8,)), dma((8,)), dma((8,)),
        dma((8,)), dma((8,)), dma((8,)), dma((8,)), dma((8,)), dma((8,)), dma((4, 2)), dma((4, 2)),
        dma(()), dma(()),
    ]
    mid = pl.pallas_call(
        functools.partial(kernel, float(2048 * 1024)),
        out_shape=(shape((2, 8, 8, 32, 256), BF16), shape((4, 16, 256), F32), shape((4, 2, 256), F32)),
        in_specs=[pl.BlockSpec(memory_space=pltpu.HBM)] * 11,
        out_specs=(pl.BlockSpec(memory_space=pltpu.VMEM),) * 3,
        scratch_shapes=scratch,
        compiler_params=pltpu.CompilerParams(
            collective_id=0, has_side_effects=True, vmem_limit_bytes=40 * 1024 * 1024
        ),
    )(*(pltpu.with_memory_space_constraint(a, pltpu.HBM) for a in args))
    mid = [pltpu.with_memory_space_constraint(m, pltpu.VMEM) for m in mid]
    whole, row, pair = shape((8, 8, 32, 256), BF16), shape((16, 256), F32), shape((2, 256), F32)
    copy_in, copy_out, *rest = pl.pallas_call(
        write_out,
        out_shape=(whole, whole) + (row,) * 4 + (pair,) * 4,
        in_specs=[pl.BlockSpec(memory_space=pltpu.VMEM)] * 3,
        out_specs=(anywhere,) * 10,
        scratch_shapes=[dma((10,))],
    )(*mid)
    return (*rest[:4], copy_in.reshape(2048, 256), copy_out.reshape(2048, 256), *rest[4:])


def solution(mesh):
    both, rows, columns = P("fs", "tp"), P("fs", None), P(None, "tp")
    return jax.shard_map(
        on_device,
        mesh=mesh,
        in_specs=(rows, both, both, rows, rows) + (both,) * 6,
        out_specs=(both,) * 4 + (columns,) * 2 + (both,) * 4,
        check_vma=False,
    )
```

```python
import functools
import math

import jax
import jax.numpy as jnp
from jax import lax
from jax.experimental import pallas as pl
from jax.experimental.pallas import tpu as pltpu
from jax.sharding import PartitionSpec as P

MESH = pl.DeviceIdType.MESH
F32 = jnp.float32
BF16 = jnp.bfloat16
FAR_FIRST = (4, 3, 5, 2, 6, 1, 7)
NEAR_FIRST = (1, 7, 2, 6, 3, 5, 4)
ROWS_FIRST = (((0,), (0,)), ((), ()))


def rank_order():
    r = lax.broadcasted_iota(jnp.int32, (256, 256), 0)
    p = lax.broadcasted_iota(jnp.int32, (256, 256), 1)
    target = ((r >> 2) & 7) * 32 + (r >> 5) * 4 + (r & 3)
    return jnp.where(target == p, 1.0, 0.0).astype(BF16)


def halves(value):
    high = value.astype(BF16)
    return high, (value - high.astype(F32)).astype(BF16)


def kernel(
    entries,
    saved, cot_in, cot_out, f_in, f_out, w_in, w_out, m1_in, m1_out, m2_in, m2_out,
    copies, rows, moments,
    s_v, c_v, fl, wl, r1, mo, mg, m1c, m2c,
    fg, go, gs, gr, spare, gh, gl, pp, rb, ab, sm, full, wg, qb, nst, nrx,
    load_sem, send_sem, a1_recv, mo_recv, w1_recv, w2_recv, near_recv, two_recv, three_recv, four_recv,
    fp_recv, wp_recv, g_recv, b2_recv, own_recv, b3_recv, c_recv, sp_recv, q_recv, n_recv,
):
    me, x = lax.axis_index("fs"), lax.axis_index("tp")
    c = lax.rem(me, 2)
    y = lax.rem(lax.div(me, 2), 8)
    z = lax.div(me, 16)
    u = z + c * (y - z)
    v = y + c * (z - y)
    other = 1 - c

    def plus(at, k):
        return lax.rem(at + k % 8, 8)

    def dev(zz, yy, cc):
        return ((zz * 8 + yy) * 2 + cc, x)

    def along_u(k, cc):
        to = plus(u, k)
        return dev(to + c * (v - to), v + c * (to - v), cc)

    def along_v(k):
        to = plus(v, k)
        return dev(u + c * (to - u), to + c * (u - to), c)

    partner = dev(z, y, other)
    sent = [0] * 7

    def send(src, dst, recv_sem, device, group):
        pltpu.make_async_remote_copy(
            src_ref=src, dst_ref=dst, send_sem=send_sem.at[group], recv_sem=recv_sem,
            device_id=device, device_id_type=MESH,
        ).start()
        sent[group] += math.prod(src.shape) * src.dtype.itemsize // 1024

    def arrive(dst, sem):
        pltpu.make_async_copy(dst, dst, sem).wait()

    barrier = pltpu.get_barrier_semaphore()
    peers = []
    for k in FAR_FIRST:
        for cc in range(2):
            peers.append(dev(plus(z, k), y, cc))
            peers.append(dev(z, plus(y, k), cc))
    for k in (2, 1, 3):
        peers.append((me, lax.rem(x + k, 4)))
        peers.append((me + 1 - 2 * c, lax.rem(x + k, 4)))
    peers.append(partner)
    for peer in peers:
        pl.semaphore_signal(barrier, inc=1, device_id=peer, device_id_type=MESH)

    def load(src, dst, group):
        copy = pltpu.make_async_copy(src, dst, load_sem.at[group])
        copy.start()
        return copy

    load(f_in, fl.at[0], 0)
    load(f_out, fl.at[1], 0)
    load(m1_in, r1.at[0], 1)
    load(m1_out, r1.at[1], 1)
    load(m2_in, r1.at[2], 1)
    load(m2_out, r1.at[3], 1)
    load(w_in, wl.at[0], 2)
    load(w_out, wl.at[1], 2)
    load(cot_in, c_v.at[:, pl.ds(pl.multiple_of(256 * c, 256), 256)], 3)
    load(cot_out, c_v.at[:, pl.ds(pl.multiple_of(256 * other, 256), 256)], 3)
    tokens = load(saved, s_v, 4)

    order = rank_order()
    arrive(fl, load_sem.at[0])
    fl[1] = jnp.dot(fl[1], order, preferred_element_type=F32).astype(BF16)
    fg[c, v, u, c] = fl[c]
    arrive(r1, load_sem.at[1])
    for X in range(2):
        mo[X, 0:2] = r1[X]
        mo[X, 2:4] = r1[2 + X]
    mg[0, y, 1] = mo[0]
    mg[1, z, 1] = mo[1]
    arrive(wl, load_sem.at[2])
    wg[c, v, u, c] = wl[c]
    pl.semaphore_wait(barrier, len(peers))

    def to_line(X, k):
        return dev(plus(z, k), y, 0) if X == 0 else dev(z, plus(y, k), 1)

    def to_cross(X, k):
        return dev(z, plus(y, k), 1) if X == 0 else dev(plus(z, k), y, 1)

    at_u, at_v = (z, y), (y, z)
    send(fl.at[other], fg.at[other, u, v, c], a1_recv.at[0], partner, 0)
    for k in FAR_FIRST:
        for X in range(2):
            send(fl.at[X], fg.at[X, at_v[X], at_u[X], c], a1_recv.at[k], to_line(X, k), 0)

    line = fg.at[c, v]

    def spread(k):
        block = line.at[plus(u, -k)]
        if k:
            arrive(block, a1_recv.at[k])
        else:
            arrive(fg.at[c, v, u, other], a1_recv.at[0])
        if k == 4:
            send(block, block, four_recv, along_v(4), 0)
            send(block, block, three_recv, along_v(3), 0)
            send(block, block, three_recv, along_v(-3), 0)
        send(block, block, two_recv.at[k], along_v(2), 0)
        send(block, block, two_recv.at[k], along_v(-2), 0)

    spread(0)
    send(wl.at[other], wg.at[other, u, v, c], w1_recv.at[0], partner, 0)
    for k in FAR_FIRST:
        for X in range(2):
            send(wl.at[X], wg.at[X, at_v[X], at_u[X], c], w1_recv.at[1], to_line(X, k), 0)

    arrive(c_v, load_sem.at[3])
    tokens.wait()

    def grad_copy(zc):
        return pltpu.make_async_remote_copy(
            src_ref=gs.at[zc], dst_ref=gr.at[zc], send_sem=send_sem.at[4], recv_sem=g_recv,
            device_id=partner, device_id_type=MESH,
        )

    def grad(zc, carry):
        at = pl.ds(pl.multiple_of(zc * 256, 256), 256)
        g = lax.dot_general(s_v[:, at], c_v[...], ROWS_FIRST, preferred_element_type=F32)
        gs[zc] = g[:, 256:512]
        go[zc] = g[:, 0:256]
        grad_copy(zc).start()
        return carry

    lax.fori_loop(0, 4, grad, 0)

    def relay(k, up):
        left, right = fg.at[c, plus(v, -2), plus(u, -k)], fg.at[c, plus(v, 2), plus(u, -k)]
        arrive(fg.at[c, v, pl.ds(0, 2)], two_recv.at[k])
        if up:
            send(left, left, four_recv, along_v(2), 0)
        else:
            send(right, right, four_recv, along_v(-2), 0)
        send(left, left, three_recv, along_v(1), 0)
        send(right, right, three_recv, along_v(-1), 0)

    def beside(k):
        block = line.at[plus(u, -k)]
        send(block, block, near_recv, along_v(1), 0)
        send(block, block, near_recv, along_v(-1), 0)

    beside(0)
    for k in (1, 7, 2, 6):
        spread(k)
        beside(k)
    relay(0, True)
    for k in (3, 5, 4):
        spread(k)

    lax.fori_loop(4, 6, grad, 0)

    for k in (1, 7, 2, 6):
        relay(k, k < 4)
    for k in (3, 5, 4):
        beside(k)
    lax.fori_loop(6, 8, grad, 0)
    for k in (3, 5):
        relay(k, k < 4)
    half = (pl.ds(0, 4), pl.ds(4, 4))

    def pass_weight(j):
        at = wg.at[c, plus(v, j)]
        send(at, at, wp_recv, partner, 3)

    def weight_step(s):
        a, b = plus(v, 1 - s), plus(v, s - 1)
        up, down = wg.at[c, a], wg.at[c, b]
        if s > 1:
            arrive(wg.at[c, pl.ds(0, 2)], w2_recv.at[s - 2])
        if s == 4:
            up, down = up.at[half[0]], down.at[half[1]]
        send(up, up, w2_recv.at[s - 1], along_v(1), 1)
        send(down, down, w2_recv.at[s - 1], along_v(-1), 1)
        pass_weight(1 - s)
        if s > 1:
            pass_weight(s - 1)

    arrive(wg.at[c, v, u, other], w1_recv.at[0])
    arrive(wg.at[c, v, pl.ds(0, 7)], w1_recv.at[1])
    weight_step(1)
    arrive(gr, g_recv)

    def combine(zc, carry):
        high, low = halves(go[zc] + gr[zc])
        for i in range(8):
            a, b = i + c * (zc - i), zc + c * (i - zc)
            gh[a, b] = high[32 * i:32 * i + 32]
            gl[a, b] = low[32 * i:32 * i + 32]
        return carry

    lax.fori_loop(0, 8, combine, 0)

    def project(j):
        f = fg[c, j].reshape(256, 256)
        term = lax.dot_general(f, gh[j].reshape(256, 256), ROWS_FIRST, preferred_element_type=F32)
        term += lax.dot_general(f, gl[j].reshape(256, 256), ROWS_FIRST, preferred_element_type=F32)
        return term.reshape(8, 32, 256)

    def pass_factor(j):
        at = fg.at[c, plus(v, j)]
        send(at, at, fp_recv, partner, 2)

    pass_factor(0)
    pp[...] = project(v)
    arrive(fg.at[c, pl.ds(0, 2)], near_recv)
    pp[...] += project(plus(v, -1))
    pp[...] += project(plus(v, 1))
    pass_factor(-1)
    pass_factor(1)
    arrive(fg.at[c, v, pl.ds(0, 2)], two_recv.at[4])
    pp[...] += project(plus(v, -2))
    pp[...] += project(plus(v, 2))
    pass_factor(-2)
    pass_factor(2)
    arrive(fg.at[c, pl.ds(0, 2)], three_recv)
    pp[...] += project(plus(v, -3))
    pp[...] += project(plus(v, 3))
    arrive(fg.at[c, 0], four_recv)
    pp[...] += project(plus(v, 4))
    for k in FAR_FIRST:
        send(pp.at[plus(u, k)], rb.at[c, u], b2_recv.at[c, k // 4 - k // 5], along_u(k, 1), 0)

    @pl.when(c == 0)
    def _():
        send(pp.at[u], rb.at[0, u], own_recv.at[0], partner, 5)
        for X in range(2):
            send(mo.at[X], mg.at[X, at_v[X], 0], mo_recv.at[0], partner, 5)

    pass_factor(-3)
    pass_factor(3)
    pass_factor(4)
    for k in FAR_FIRST:
        for X in range(2):
            send(mo.at[X], mg.at[X, at_v[X], c], mo_recv.at[1], to_cross(X, k), 0)

    weight_step(2)

    @pl.when(c == 1)
    def _():
        for X in (1, 0):
            arrive(rb.at[X, pl.ds(0, 6)], b2_recv.at[X, 0])
            arrive(rb.at[X, 0], b2_recv.at[X, 1])
            if X == 0:
                arrive(rb.at[0, 0], own_recv.at[0])
            total = rb[0, z] if X == 0 else pp[y]
            for k in NEAR_FIRST:
                total += rb[X, plus(at_u[X], -k)]
            mine = ab.at[X, at_v[X]]
            mine[...] = total
            for k in FAR_FIRST:
                send(mine, mine, b3_recv.at[X], to_cross(X, k), 6)
        arrive(mg.at[0, 0], mo_recv.at[0])
        arrive(mg.at[:, pl.ds(0, 7)], mo_recv.at[1])
        for X in range(2):
            for k in range(8):
                for cc in range(2):
                    at = 4 * k + 2 * cc
                    m1c[X, at:at + 2] = mg[X, k, cc, 0:2]
                    m2c[X, at:at + 2] = mg[X, k, cc, 2:4]

    weight_step(3)

    @pl.when(c == 1)
    def _():
        for X in (1, 0):
            arrive(ab.at[X, pl.ds(0, 7)], b3_recv.at[X])
            projected = ab[X, 0]
            for k in range(1, 8):
                projected += ab[X, k]
            first = 0.8 * m1c[X] + 0.2 * projected
            second = 0.9 * m2c[X] + 0.1 * projected * projected
            mine = sm.at[X, at_u[X]]
            mine[...] = first / (jnp.sqrt(second) + 1e-08)
            for k in FAR_FIRST:
                send(mine, mine, c_recv.at[min(k, 8 - k) - 1], to_line(X, k), 6)
            send(mine, mine, own_recv.at[1], partner, 6)
            m1c[X] = first
            m2c[X] = second
        for X in range(2):
            for i in range(2):
                at = 4 * at_v[X] + i
                nst[4 * X + i:4 * X + i + 1] = m1c[X, pl.ds(at, 1)]
                nst[4 * X + 2 + i:4 * X + 3 + i] = m2c[X, pl.ds(at, 1)]
                moments[X, i:i + 1] = m1c[X, pl.ds(at + 2, 1)]
                moments[2 + X, i:i + 1] = m2c[X, pl.ds(at + 2, 1)]
        send(nst, nrx, n_recv, partner, 6)

    weight_step(4)

    @pl.when(c == 0)
    def _():
        arrive(sm.at[0, pl.ds(0, 2)], own_recv.at[1])

    for k in (1, 2, 3, 4):
        pair = (k, -k) if k < 4 else (4,)
        arrive(sm.at[c, pl.ds(0, len(pair))], c_recv.at[k - 1])
        for i in pair:
            at = sm.at[c, plus(u, i)]
            send(at, at, sp_recv, partner, 2)

    def expanded(X):
        high, low = halves(sm[X].reshape(256, 256))
        small = jnp.concatenate([high, low], axis=0)

        def expand(j, squares):
            f = fg[X, j].reshape(256, 256)
            value = jnp.dot(jnp.concatenate([f, f], axis=1), small, preferred_element_type=F32)
            full[X, j] = value.reshape(8, 2, 16, 256)
            return squares + jnp.sum((value * value).reshape(32, 8, 256), axis=0)

        return lax.fori_loop(0, 8, expand, jnp.zeros((8, 256), F32), unroll=2)

    squares = expanded(c)
    qb[4 * c + x] = jnp.broadcast_to(jnp.sum(squares, keepdims=True), (8, 128))
    mine = qb.at[4 * c + x]
    for k in (2, 1, 3):
        to = lax.rem(x + k, 4)
        send(mine, mine, q_recv, (me, to), 2)
        send(mine, mine, q_recv, (me + 1 - 2 * c, to), 2)
    send(mine, mine, q_recv, partner, 2)
    four = wg.at[c, plus(v, 4)]
    arrive(four, w2_recv.at[3])
    pass_weight(4)
    arrive(fg.at[other], fp_recv)
    arrive(sm.at[other, pl.ds(0, 7)], sp_recv)
    expanded(other)
    arrive(qb.at[pl.ds(0, 7)], q_recv)

    def scale_of(X):
        square = ((qb[4 * X] + qb[4 * X + 1]) + qb[4 * X + 2]) + qb[4 * X + 3]
        scale = 1.0 / jnp.sqrt(square[0:1] / entries + 1e-06)
        return jnp.concatenate([scale, scale], axis=1)

    def finish(X, first_line, last_line):
        scale = scale_of(X)

        def line(j, carry):
            update = full[X, j].reshape(256, 256) * scale
            fresh = wg[X, j].reshape(256, 256) - 0.02 * update
            rounded = fresh.astype(BF16)
            for i in range(8):
                copies[X, i + X * (j - i), j + X * (i - j)] = rounded[32 * i:32 * i + 32]
            return carry

        lax.fori_loop(first_line, last_line, line, 0)

    finish(c, 0, 8)
    for X in range(2):
        update = full[X, at_v[X], at_u[X], c] * scale_of(X)
        rows[X] = update
        rows[2 + X] = wl[X] - 0.02 * update

    @pl.when(c == 0)
    def _():
        arrive(nrx, n_recv)
        for X in range(2):
            moments[X] = nrx[4 * X:4 * X + 2]
            moments[2 + X] = nrx[4 * X + 2:4 * X + 4]

    arrive(wg.at[other], wp_recv)
    finish(other, 0, 8)
    sent[4] = 2048

    def drained(group):
        arrive(spare.at[pl.ds(0, sent[group] // 4)], send_sem.at[group])

    for group in range(5):
        drained(group)
    pl.when(c == 0)(lambda: drained(5))
    pl.when(c == 1)(lambda: drained(6))


def write_out(copies, rows, moments, *refs):
    outs, sems = refs[:-1], refs[-1]
    sources = [copies.at[0], copies.at[1]] + [rows.at[i] for i in range(4)] + [moments.at[i] for i in range(4)]
    writes = [pltpu.make_async_copy(src, dst, sems.at[i]) for i, (src, dst) in enumerate(zip(sources, outs))]
    for write in writes:
        write.start()
    for write in writes:
        write.wait()


def on_device(*args):
    shape = jax.ShapeDtypeStruct
    dma = pltpu.SemaphoreType.DMA
    vmem = pltpu.VMEM
    anywhere = pl.BlockSpec(memory_space=pl.ANY)
    scratch = [
        vmem((768, 2048), BF16), vmem((768, 512), BF16),
        vmem((2, 16, 256), BF16), vmem((2, 16, 256), F32), vmem((4, 2, 256), F32),
        vmem((2, 8, 256), F32), vmem((2, 8, 2, 8, 256), F32),
        vmem((2, 32, 256), F32), vmem((2, 32, 256), F32),
        vmem((2, 8, 8, 2, 16, 256), BF16),
        vmem((8, 256, 256), F32), vmem((8, 256, 256), F32), vmem((8, 256, 256), F32), vmem((512, 8, 128), F32),
        vmem((8, 8, 32, 256), BF16), vmem((8, 8, 32, 256), BF16),
        vmem((8, 32, 256), F32), vmem((2, 8, 32, 256), F32),
        vmem((2, 8, 32, 256), F32), vmem((2, 8, 32, 256), F32),
        vmem((2, 8, 8, 2, 16, 256), F32), vmem((2, 8, 8, 2, 16, 256), F32),
        vmem((8, 8, 128), F32), vmem((8, 256), F32), vmem((8, 256), F32),
        dma((5,)), dma((7,)), dma((8,)), dma((2,)), dma((2,)), dma((4,)), dma(()), dma((8,)), dma(()), dma(()),
        dma(()), dma(()), dma(()), dma((2, 2)), dma((2,)), dma((2,)), dma((4,)), dma(()), dma(()), dma(()),
    ]
    mid = pl.pallas_call(
        functools.partial(kernel, float(2048 * 1024)),
        out_shape=(shape((2, 8, 8, 32, 256), BF16), shape((4, 16, 256), F32), shape((4, 2, 256), F32)),
        in_specs=[pl.BlockSpec(memory_space=pltpu.HBM)] * 11,
        out_specs=(pl.BlockSpec(memory_space=pltpu.VMEM),) * 3,
        scratch_shapes=scratch,
        compiler_params=pltpu.CompilerParams(
            collective_id=0, has_side_effects=True, vmem_limit_bytes=40 * 1024 * 1024
        ),
    )(*(pltpu.with_memory_space_constraint(a, pltpu.HBM) for a in args))
    mid = [pltpu.with_memory_space_constraint(m, pltpu.VMEM) for m in mid]
    whole, row, pair = shape((8, 8, 32, 256), BF16), shape((16, 256), F32), shape((2, 256), F32)
    copy_in, copy_out, *rest = pl.pallas_call(
        write_out,
        out_shape=(whole, whole) + (row,) * 4 + (pair,) * 4,
        in_specs=[pl.BlockSpec(memory_space=pltpu.VMEM)] * 3,
        out_specs=(anywhere,) * 10,
        scratch_shapes=[dma((10,))],
    )(*mid)
    return (*rest[:4], copy_in.reshape(2048, 256), copy_out.reshape(2048, 256), *rest[4:])


def solution(mesh):
    both, rows, columns = P("fs", "tp"), P("fs", None), P(None, "tp")
    return jax.shard_map(
        on_device,
        mesh=mesh,
        in_specs=(rows, both, both, rows, rows) + (both,) * 6,
        out_specs=(both,) * 4 + (columns,) * 2 + (both,) * 4,
        check_vma=False,
    )
```

```python
import functools
import math

import jax
import jax.numpy as jnp
from jax import lax
from jax.experimental import pallas as pl
from jax.experimental.pallas import tpu as pltpu
from jax.sharding import PartitionSpec as P

MESH = pl.DeviceIdType.MESH
F32 = jnp.float32
BF16 = jnp.bfloat16
FAR_FIRST = (4, 3, 5, 2, 6, 1, 7)
NEAR_FIRST = (1, 7, 2, 6, 3, 5, 4)
ROWS_FIRST = (((0,), (0,)), ((), ()))


def rank_order():
    r = lax.broadcasted_iota(jnp.int32, (256, 256), 0)
    p = lax.broadcasted_iota(jnp.int32, (256, 256), 1)
    target = ((r >> 2) & 7) * 32 + (r >> 5) * 4 + (r & 3)
    return jnp.where(target == p, 1.0, 0.0).astype(BF16)


def halves(value):
    high = value.astype(BF16)
    return high, (value - high.astype(F32)).astype(BF16)


def thirds(value):
    high = value.astype(BF16)
    rest = value - high.astype(F32)
    middle = rest.astype(BF16)
    return high, middle, (rest - middle.astype(F32)).astype(BF16)


def kernel(
    saved, cot_in, cot_out, f_in, f_out, w_in, w_out, m1_in, m1_out, m2_in, m2_out,
    full, wg, qb, moments,
    s_v, c_v, fl, wl, r1, mo, mg, m1c, m2c,
    fg, go, gs, gr, spare, gh, gl, pp, rb, ab, sm, nst, nrx, gm,
    load_sem, send_sem, a1_recv, mo_recv, w1_recv, w2_recv, near_recv, two_recv, three_recv, four_recv,
    fp_recv, wp_recv, g_recv, b2_recv, own_recv, b3_recv, c_recv, sp_recv, q_recv, n_recv,
):
    me, x = lax.axis_index("fs"), lax.axis_index("tp")
    c = lax.rem(me, 2)
    y = lax.rem(lax.div(me, 2), 8)
    z = lax.div(me, 16)
    u = z + c * (y - z)
    v = y + c * (z - y)
    other = 1 - c

    def plus(at, k):
        return lax.rem(at + k % 8, 8)

    def dev(zz, yy, cc):
        return ((zz * 8 + yy) * 2 + cc, x)

    def along_u(k, cc):
        to = plus(u, k)
        return dev(to + c * (v - to), v + c * (to - v), cc)

    def along_v(k):
        to = plus(v, k)
        return dev(u + c * (to - u), to + c * (u - to), c)

    partner = dev(z, y, other)
    sent = [0] * 7

    def send(src, dst, recv_sem, device, group):
        pltpu.make_async_remote_copy(
            src_ref=src, dst_ref=dst, send_sem=send_sem.at[group], recv_sem=recv_sem,
            device_id=device, device_id_type=MESH,
        ).start()
        sent[group] += math.prod(src.shape) * src.dtype.itemsize // 1024

    def arrive(dst, sem):
        pltpu.make_async_copy(dst, dst, sem).wait()

    barrier = pltpu.get_barrier_semaphore()
    peers = []
    for k in FAR_FIRST:
        for cc in range(2):
            peers.append(dev(plus(z, k), y, cc))
            peers.append(dev(z, plus(y, k), cc))
    for k in (2, 1, 3):
        peers.append((me, lax.rem(x + k, 4)))
        peers.append((me + 1 - 2 * c, lax.rem(x + k, 4)))
    peers.append(partner)
    for peer in peers:
        pl.semaphore_signal(barrier, inc=1, device_id=peer, device_id_type=MESH)

    def load(src, dst, group):
        copy = pltpu.make_async_copy(src, dst, load_sem.at[group])
        copy.start()
        return copy

    load(f_in, fl.at[0], 0)
    load(f_out, fl.at[1], 0)
    load(m1_in, r1.at[0], 1)
    load(m1_out, r1.at[1], 1)
    load(m2_in, r1.at[2], 1)
    load(m2_out, r1.at[3], 1)
    load(w_in, wl.at[0], 2)
    load(w_out, wl.at[1], 2)
    load(cot_in, c_v.at[:, pl.ds(pl.multiple_of(256 * c, 256), 256)], 3)
    load(cot_out, c_v.at[:, pl.ds(pl.multiple_of(256 * other, 256), 256)], 3)
    tokens = load(saved, s_v, 4)

    order = rank_order()
    arrive(fl, load_sem.at[0])
    fl[1] = jnp.dot(fl[1], order, preferred_element_type=F32).astype(BF16)
    fg[c, v, u, c] = fl[c]
    arrive(r1, load_sem.at[1])
    for X in range(2):
        mo[X, 0:2] = r1[X]
        mo[X, 2:4] = r1[2 + X]
    mg[0, y, 1] = mo[0]
    mg[1, z, 1] = mo[1]
    arrive(wl, load_sem.at[2])
    wg[c, v, u, c] = wl[c]
    pl.semaphore_wait(barrier, len(peers))

    def to_line(X, k):
        return dev(plus(z, k), y, 0) if X == 0 else dev(z, plus(y, k), 1)

    def to_cross(X, k):
        return dev(z, plus(y, k), 1) if X == 0 else dev(plus(z, k), y, 1)

    at_u, at_v = (z, y), (y, z)
    send(fl.at[other], fg.at[other, u, v, c], a1_recv.at[0], partner, 0)
    for k in FAR_FIRST:
        for X in range(2):
            send(fl.at[X], fg.at[X, at_v[X], at_u[X], c], a1_recv.at[k], to_line(X, k), 0)

    line = fg.at[c, v]

    def spread(k):
        block = line.at[plus(u, -k)]
        if k:
            arrive(block, a1_recv.at[k])
        else:
            arrive(fg.at[c, v, u, other], a1_recv.at[0])
        if k == 4:
            send(block, block, four_recv, along_v(4), 0)
            send(block, block, three_recv, along_v(3), 0)
            send(block, block, three_recv, along_v(-3), 0)
        send(block, block, two_recv.at[k], along_v(2), 0)
        send(block, block, two_recv.at[k], along_v(-2), 0)

    spread(0)
    send(wl.at[other], wg.at[other, u, v, c], w1_recv.at[0], partner, 0)
    for k in FAR_FIRST:
        for X in range(2):
            send(wl.at[X], wg.at[X, at_v[X], at_u[X], c], w1_recv.at[1], to_line(X, k), 0)

    arrive(c_v, load_sem.at[3])
    tokens.wait()

    def grad_copy(zc):
        return pltpu.make_async_remote_copy(
            src_ref=gs.at[zc], dst_ref=gr.at[zc], send_sem=send_sem.at[4], recv_sem=g_recv,
            device_id=partner, device_id_type=MESH,
        )

    def grad(zc, carry):
        at = pl.ds(pl.multiple_of(zc * 256, 256), 256)
        g = lax.dot_general(s_v[:, at], c_v[...], ROWS_FIRST, preferred_element_type=F32)
        gs[zc] = g[:, 256:512]
        go[zc] = g[:, 0:256]
        grad_copy(zc).start()
        return carry

    lax.fori_loop(0, 4, grad, 0)

    def relay(k, up):
        left, right = fg.at[c, plus(v, -2), plus(u, -k)], fg.at[c, plus(v, 2), plus(u, -k)]
        arrive(fg.at[c, v, pl.ds(0, 2)], two_recv.at[k])
        if up:
            send(left, left, four_recv, along_v(2), 0)
        else:
            send(right, right, four_recv, along_v(-2), 0)
        send(left, left, three_recv, along_v(1), 0)
        send(right, right, three_recv, along_v(-1), 0)

    def beside(k):
        block = line.at[plus(u, -k)]
        send(block, block, near_recv, along_v(1), 0)
        send(block, block, near_recv, along_v(-1), 0)

    beside(0)
    for k in (1, 7, 2, 6):
        spread(k)
        beside(k)
    relay(0, True)
    for k in (3, 5, 4):
        spread(k)
    for k in (3, 5, 4):
        beside(k)

    lax.fori_loop(4, 8, grad, 0)

    for k in (1, 7, 2, 6):
        relay(k, k < 4)
    for k in (3, 5):
        relay(k, k < 4)
    for k in FAR_FIRST:
        for X in range(2):
            send(mo.at[X], mg.at[X, at_v[X], c], mo_recv.at[1], to_cross(X, k), 0)

    @pl.when(c == 0)
    def _():
        for X in range(2):
            send(mo.at[X], mg.at[X, at_v[X], 0], mo_recv.at[0], partner, 5)

    parts = [pl.ds(2 * i, 2) for i in range(4)]

    def pass_weight(j):
        at = wg.at[c, plus(v, j)]
        send(at, at, wp_recv, partner, 3)

    def weight_step(s):
        a, b = plus(v, 1 - s), plus(v, s - 1)
        up, down = wg.at[c, a], wg.at[c, b]
        for i, part in enumerate(parts):
            if s > 1:
                arrive(wg.at[c, v, pl.ds(0, 4)], w2_recv.at[s - 2, i])
            if s < 4 or i < 2:
                send(up.at[part], up.at[part], w2_recv.at[s - 1, i], along_v(1), 1)
            if s < 4 or i > 1:
                send(down.at[part], down.at[part], w2_recv.at[s - 1, i], along_v(-1), 1)
        pass_weight(1 - s)
        if s > 1:
            pass_weight(s - 1)

    arrive(wg.at[c, v, u, other], w1_recv.at[0])
    arrive(wg.at[c, v, pl.ds(0, 7)], w1_recv.at[1])
    weight_step(1)
    arrive(gr, g_recv)

    def combine(zc, carry):
        high, low = halves(go[zc] + gr[zc])
        for i in range(8):
            a, b = i + c * (zc - i), zc + c * (i - zc)
            gh[a, b] = high[32 * i:32 * i + 32]
            gl[a, b] = low[32 * i:32 * i + 32]
        return carry

    lax.fori_loop(0, 8, combine, 0)

    def project(j):
        f = fg[c, j].reshape(256, 256)
        term = lax.dot_general(f, gh[j].reshape(256, 256), ROWS_FIRST, preferred_element_type=F32)
        term += lax.dot_general(f, gl[j].reshape(256, 256), ROWS_FIRST, preferred_element_type=F32)
        return term.reshape(8, 32, 256)

    def pass_factor(j):
        at = fg.at[c, plus(v, j)]
        send(at, at, fp_recv, partner, 2)

    pass_factor(0)
    pp[...] = project(v)
    arrive(fg.at[c, pl.ds(0, 2)], near_recv)
    pp[...] += project(plus(v, -1))
    pp[...] += project(plus(v, 1))
    pass_factor(-1)
    pass_factor(1)
    arrive(fg.at[c, v, pl.ds(0, 2)], two_recv.at[4])
    pp[...] += project(plus(v, -2))
    pp[...] += project(plus(v, 2))
    pass_factor(-2)
    pass_factor(2)
    arrive(fg.at[c, pl.ds(0, 2)], three_recv)
    pp[...] += project(plus(v, -3))
    pp[...] += project(plus(v, 3))
    arrive(fg.at[c, 0], four_recv)
    pp[...] += project(plus(v, 4))
    for k in FAR_FIRST:
        send(pp.at[plus(u, k)], rb.at[c, u], b2_recv.at[c, k // 4 - k // 5], along_u(k, 1), 0)

    @pl.when(c == 0)
    def _():
        send(pp.at[u], rb.at[0, u], own_recv.at[0], partner, 5)

    pass_factor(-3)
    pass_factor(3)
    pass_factor(4)
    def squared(j, total):
        f = fg[c, j].reshape(256, 256)
        return total + lax.dot_general(f, f, ROWS_FIRST, preferred_element_type=F32)

    gram = lax.fori_loop(0, 8, squared, jnp.zeros((256, 256), F32))
    for i, part in enumerate(thirds(gram)):
        for at in ((0, 256, 1024), (512, 768), (1280,))[i]:
            gm[:, at:at + 256] = part
    weight_step(2)

    @pl.when(c == 1)
    def _():
        for X in (1, 0):
            arrive(rb.at[X, pl.ds(0, 6)], b2_recv.at[X, 0])
            arrive(rb.at[X, 0], b2_recv.at[X, 1])
            if X == 0:
                arrive(rb.at[0, 0], own_recv.at[0])
            total = rb[0, z] if X == 0 else pp[y]
            for k in NEAR_FIRST:
                total += rb[X, plus(at_u[X], -k)]
            mine = ab.at[X, at_v[X]]
            mine[...] = total
            for k in FAR_FIRST:
                send(mine, mine, b3_recv.at[X], to_cross(X, k), 6)
        arrive(mg.at[0, 0], mo_recv.at[0])
        arrive(mg.at[:, pl.ds(0, 7)], mo_recv.at[1])
        for X in range(2):
            for k in range(8):
                for cc in range(2):
                    at = 4 * k + 2 * cc
                    m1c[X, at:at + 2] = mg[X, k, cc, 0:2]
                    m2c[X, at:at + 2] = mg[X, k, cc, 2:4]

    weight_step(3)

    @pl.when(c == 1)
    def _():
        for X in (1, 0):
            arrive(ab.at[X, pl.ds(0, 7)], b3_recv.at[X])
            projected = ab[X, 0]
            for k in range(1, 8):
                projected += ab[X, k]
            first = 0.8 * m1c[X] + 0.2 * projected
            second = 0.9 * m2c[X] + 0.1 * projected * projected
            mine = sm.at[X, at_u[X]]
            mine[...] = first / (jnp.sqrt(second) + 1e-08)
            for k in FAR_FIRST:
                send(mine, mine, c_recv.at[min(k, 8 - k) - 1], to_line(X, k), 6)
            send(mine, mine, own_recv.at[1], partner, 6)
            m1c[X] = first
            m2c[X] = second
        for X in range(2):
            for i in range(2):
                at = 4 * at_v[X] + i
                nst[4 * X + i:4 * X + i + 1] = m1c[X, pl.ds(at, 1)]
                nst[4 * X + 2 + i:4 * X + 3 + i] = m2c[X, pl.ds(at, 1)]
                moments[X, i:i + 1] = m1c[X, pl.ds(at + 2, 1)]
                moments[2 + X, i:i + 1] = m2c[X, pl.ds(at + 2, 1)]
        send(nst, nrx, n_recv, partner, 6)

    weight_step(4)

    @pl.when(c == 0)
    def _():
        arrive(sm.at[0, pl.ds(0, 2)], own_recv.at[1])

    for k in (1, 2, 3, 4):
        pair = (k, -k) if k < 4 else (4,)
        arrive(sm.at[c, pl.ds(0, len(pair))], c_recv.at[k - 1])
        for i in pair:
            at = sm.at[c, plus(u, i)]
            send(at, at, sp_recv, partner, 2)

    small = sm[c].reshape(256, 256)
    high, middle, low = thirds(small)
    spread_small = jnp.concatenate([high, middle, high, middle, low, high], axis=0)
    squares = small * jnp.dot(gm[...], spread_small, preferred_element_type=F32)
    qb[4 * c + x] = jnp.broadcast_to(jnp.sum(squares, keepdims=True), (8, 128))
    mine = qb.at[4 * c + x]
    for k in (2, 1, 3):
        to = lax.rem(x + k, 4)
        send(mine, mine, q_recv, (me, to), 2)
        send(mine, mine, q_recv, (me + 1 - 2 * c, to), 2)
    send(mine, mine, q_recv, partner, 2)

    def expanded(X):
        high, low = halves(sm[X].reshape(256, 256))
        small = jnp.concatenate([high, low], axis=0)

        def expand(j, carry):
            f = fg[X, j].reshape(256, 256)
            value = jnp.dot(jnp.concatenate([f, f], axis=1), small, preferred_element_type=F32)
            full[X, j] = value.reshape(8, 2, 16, 256)
            return carry

        lax.fori_loop(0, 8, expand, 0, unroll=2)

    expanded(c)
    four = wg.at[c, plus(v, 4)]
    for i, part in enumerate(parts):
        arrive(four.at[part], w2_recv.at[3, i])
    pass_weight(4)
    arrive(fg.at[other], fp_recv)
    arrive(sm.at[other, pl.ds(0, 7)], sp_recv)
    expanded(other)
    arrive(qb.at[pl.ds(0, 7)], q_recv)

    @pl.when(c == 0)
    def _():
        arrive(nrx, n_recv)
        for X in range(2):
            moments[X] = nrx[4 * X:4 * X + 2]
            moments[2 + X] = nrx[4 * X + 2:4 * X + 4]

    arrive(wg.at[other], wp_recv)
    sent[4] = 2048

    def drained(group):
        arrive(spare.at[pl.ds(0, sent[group] // 4)], send_sem.at[group])

    for group in range(5):
        drained(group)
    pl.when(c == 0)(lambda: drained(5))
    pl.when(c == 1)(lambda: drained(6))


def write_out(
    entries, full, wg, qb, moments,
    copy_in, copy_out, upd_in, upd_out, new_in, new_out, fst_in, fst_out, snd_in, snd_out,
    copies, rows, sems,
):
    me = lax.axis_index("fs")
    c = lax.rem(me, 2)
    y = lax.rem(lax.div(me, 2), 8)
    z = lax.div(me, 16)
    writes = []

    def write(src, dst):
        writes.append(pltpu.make_async_copy(src, dst, sems.at[len(writes)]))
        writes[-1].start()

    for i, dst in enumerate((fst_in, fst_out, snd_in, snd_out)):
        write(moments.at[i], dst)
    for X in range(2):
        square = ((qb[4 * X] + qb[4 * X + 1]) + qb[4 * X + 2]) + qb[4 * X + 3]
        scale = 1.0 / jnp.sqrt(square[0:1] / entries + 1e-06)
        scale = jnp.concatenate([scale, scale], axis=1)

        def line(j, carry):
            update = full[X, j].reshape(256, 256) * scale
            fresh = wg[X, j].reshape(256, 256) - 0.02 * update
            copies[X, j] = fresh.astype(BF16).reshape(8, 32, 256)
            dst = copy_out.at[j] if X else copy_in.at[:, j]
            pltpu.make_async_copy(copies.at[X, j], dst, sems.at[8 + X]).start()
            return carry

        lax.fori_loop(0, 8, line, 0)
        at = (z, y, c) if X else (y, z, c)
        update = full[X, at[0], at[1], at[2]] * scale
        rows[X] = update
        rows[2 + X] = wg[X, at[0], at[1], at[2]] - 0.02 * update
        write(rows.at[X], upd_out if X else upd_in)
        write(rows.at[2 + X], new_out if X else new_in)
    for copy in writes:
        copy.wait()
    for X in range(2):
        pltpu.make_async_copy(copies.at[X], copies.at[X], sems.at[8 + X]).wait()


def on_device(*args):
    shape = jax.ShapeDtypeStruct
    dma = pltpu.SemaphoreType.DMA
    vmem = pltpu.VMEM
    anywhere = pl.BlockSpec(memory_space=pl.ANY)
    scratch = [
        vmem((768, 2048), BF16), vmem((768, 512), BF16),
        vmem((2, 16, 256), BF16), vmem((2, 16, 256), F32), vmem((4, 2, 256), F32),
        vmem((2, 4, 256), F32), vmem((2, 8, 2, 4, 256), F32),
        vmem((2, 32, 256), F32), vmem((2, 32, 256), F32),
        vmem((2, 8, 8, 2, 16, 256), BF16),
        vmem((8, 256, 256), F32), vmem((8, 256, 256), F32), vmem((8, 256, 256), F32), vmem((512, 8, 128), F32),
        vmem((8, 8, 32, 256), BF16), vmem((8, 8, 32, 256), BF16),
        vmem((8, 32, 256), F32), vmem((2, 8, 32, 256), F32),
        vmem((2, 8, 32, 256), F32), vmem((2, 8, 32, 256), F32),
        vmem((8, 256), F32), vmem((8, 256), F32), vmem((256, 1536), BF16),
        dma((5,)), dma((7,)), dma((8,)), dma((2,)), dma((2,)), dma((4, 4)), dma(()), dma((8,)), dma(()), dma(()),
        dma(()), dma(()), dma(()), dma((2, 2)), dma((2,)), dma((2,)), dma((4,)), dma(()), dma(()), dma(()),
    ]
    lines = shape((2, 8, 8, 2, 16, 256), F32)
    mid = pl.pallas_call(
        kernel,
        out_shape=(lines, lines, shape((8, 8, 128), F32), shape((4, 2, 256), F32)),
        in_specs=[pl.BlockSpec(memory_space=pltpu.HBM)] * 11,
        out_specs=(pl.BlockSpec(memory_space=pltpu.VMEM),) * 4,
        scratch_shapes=scratch,
        compiler_params=pltpu.CompilerParams(
            collective_id=0, has_side_effects=True, vmem_limit_bytes=40 * 1024 * 1024
        ),
    )(*(pltpu.with_memory_space_constraint(a, pltpu.HBM) for a in args))
    mid = [pltpu.with_memory_space_constraint(m, pltpu.VMEM) for m in mid]
    whole, row, pair = shape((8, 8, 32, 256), BF16), shape((16, 256), F32), shape((2, 256), F32)
    copy_in, copy_out, *rest = pl.pallas_call(
        functools.partial(write_out, float(2048 * 1024)),
        out_shape=(whole, whole) + (row,) * 4 + (pair,) * 4,
        in_specs=[pl.BlockSpec(memory_space=pltpu.VMEM)] * 4,
        out_specs=(anywhere,) * 10,
        scratch_shapes=[vmem((2, 8, 8, 32, 256), BF16), vmem((4, 16, 256), F32), dma((10,))],
        compiler_params=pltpu.CompilerParams(vmem_limit_bytes=16 * 1024 * 1024),
    )(*mid)
    return (*rest[:4], copy_in.reshape(2048, 256), copy_out.reshape(2048, 256), *rest[4:])


def solution(mesh):
    both, rows, columns = P("fs", "tp"), P("fs", None), P(None, "tp")
    return jax.shard_map(
        on_device,
        mesh=mesh,
        in_specs=(rows, both, both, rows, rows) + (both,) * 6,
        out_specs=(both,) * 4 + (columns,) * 2 + (both,) * 4,
        check_vma=False,
    )
```

```python
import functools
import math

import jax
import jax.numpy as jnp
from jax import lax
from jax.experimental import pallas as pl
from jax.experimental.pallas import tpu as pltpu
from jax.sharding import PartitionSpec as P

MESH = pl.DeviceIdType.MESH
F32 = jnp.float32
BF16 = jnp.bfloat16
FAR_FIRST = (4, 3, 5, 2, 6, 1, 7)
NEAR_FIRST = (1, 7, 2, 6, 3, 5, 4)
ROWS_FIRST = (((0,), (0,)), ((), ()))


def rank_order():
    r = lax.broadcasted_iota(jnp.int32, (256, 256), 0)
    p = lax.broadcasted_iota(jnp.int32, (256, 256), 1)
    target = ((r >> 2) & 7) * 32 + (r >> 5) * 4 + (r & 3)
    return jnp.where(target == p, 1.0, 0.0).astype(BF16)


def halves(value):
    high = value.astype(BF16)
    return high, (value - high.astype(F32)).astype(BF16)


def thirds(value):
    high = value.astype(BF16)
    rest = value - high.astype(F32)
    middle = rest.astype(BF16)
    return high, middle, (rest - middle.astype(F32)).astype(BF16)


def kernel(
    saved, cot_in, cot_out, f_in, f_out, w_in, w_out, m1_in, m1_out, m2_in, m2_out,
    full, wg, qb, moments,
    s_v, c_v, fl, wl, r1, mo, mg, m1c, m2c,
    fg, go, gs, gr, spare, gh, gl, pp, rb, ab, sm, nst, nrx, gm,
    load_sem, send_sem, a1_recv, mo_recv, w1_recv, w2_recv, near_recv, two_recv, three_recv, four_recv,
    fp_recv, wp_recv, g_recv, b2_recv, own_recv, b3_recv, c_recv, sp_recv, q_recv, n_recv,
):
    me, x = lax.axis_index("fs"), lax.axis_index("tp")
    c = lax.rem(me, 2)
    y = lax.rem(lax.div(me, 2), 8)
    z = lax.div(me, 16)
    u = z + c * (y - z)
    v = y + c * (z - y)
    other = 1 - c

    def plus(at, k):
        return lax.rem(at + k % 8, 8)

    def dev(zz, yy, cc):
        return ((zz * 8 + yy) * 2 + cc, x)

    def along_u(k, cc):
        to = plus(u, k)
        return dev(to + c * (v - to), v + c * (to - v), cc)

    def along_v(k):
        to = plus(v, k)
        return dev(u + c * (to - u), to + c * (u - to), c)

    partner = dev(z, y, other)
    sent = [0] * 7

    def send(src, dst, recv_sem, device, group):
        pltpu.make_async_remote_copy(
            src_ref=src, dst_ref=dst, send_sem=send_sem.at[group], recv_sem=recv_sem,
            device_id=device, device_id_type=MESH,
        ).start()
        sent[group] += math.prod(src.shape) * src.dtype.itemsize // 1024

    def arrive(dst, sem):
        pltpu.make_async_copy(dst, dst, sem).wait()

    barrier = pltpu.get_barrier_semaphore()
    peers = []
    for k in FAR_FIRST:
        for cc in range(2):
            peers.append(dev(plus(z, k), y, cc))
            peers.append(dev(z, plus(y, k), cc))
    for k in (2, 1, 3):
        peers.append((me, lax.rem(x + k, 4)))
        peers.append((me + 1 - 2 * c, lax.rem(x + k, 4)))
    peers.append(partner)
    for peer in peers:
        pl.semaphore_signal(barrier, inc=1, device_id=peer, device_id_type=MESH)

    def load(src, dst, group):
        copy = pltpu.make_async_copy(src, dst, load_sem.at[group])
        copy.start()
        return copy

    load(f_in, fl.at[0], 0)
    load(f_out, fl.at[1], 0)
    load(m1_in, r1.at[0], 1)
    load(m1_out, r1.at[1], 1)
    load(m2_in, r1.at[2], 1)
    load(m2_out, r1.at[3], 1)
    load(w_in, wl.at[0], 2)
    load(w_out, wl.at[1], 2)
    load(cot_in, c_v.at[:, pl.ds(pl.multiple_of(256 * c, 256), 256)], 3)
    load(cot_out, c_v.at[:, pl.ds(pl.multiple_of(256 * other, 256), 256)], 3)
    tokens = load(saved, s_v, 4)

    order = rank_order()
    arrive(fl, load_sem.at[0])
    fl[1] = jnp.dot(fl[1], order, preferred_element_type=F32).astype(BF16)
    fg[c, v, u, c] = fl[c]
    arrive(r1, load_sem.at[1])
    for X in range(2):
        mo[X, 0:2] = r1[X]
        mo[X, 2:4] = r1[2 + X]
    mg[0, y, 1] = mo[0]
    mg[1, z, 1] = mo[1]
    arrive(wl, load_sem.at[2])
    wg[c, v, u, c] = wl[c]
    pl.semaphore_wait(barrier, len(peers))

    def to_line(X, k):
        return dev(plus(z, k), y, 0) if X == 0 else dev(z, plus(y, k), 1)

    def to_cross(X, k):
        return dev(z, plus(y, k), 1) if X == 0 else dev(plus(z, k), y, 1)

    at_u, at_v = (z, y), (y, z)
    send(fl.at[other], fg.at[other, u, v, c], a1_recv.at[0], partner, 0)
    for k in FAR_FIRST:
        for X in range(2):
            send(fl.at[X], fg.at[X, at_v[X], at_u[X], c], a1_recv.at[k], to_line(X, k), 0)

    line = fg.at[c, v]

    def spread(k):
        block = line.at[plus(u, -k)]
        if k:
            arrive(block, a1_recv.at[k])
        else:
            arrive(fg.at[c, v, u, other], a1_recv.at[0])
        if k == 4:
            send(block, block, four_recv, along_v(4), 0)
            send(block, block, three_recv, along_v(3), 0)
            send(block, block, three_recv, along_v(-3), 0)
        send(block, block, two_recv.at[k], along_v(2), 0)
        send(block, block, two_recv.at[k], along_v(-2), 0)

    spread(0)
    send(wl.at[other], wg.at[other, u, v, c], w1_recv.at[0], partner, 0)
    for k in FAR_FIRST:
        for X in range(2):
            send(wl.at[X], wg.at[X, at_v[X], at_u[X], c], w1_recv.at[1], to_line(X, k), 0)

    arrive(c_v, load_sem.at[3])
    tokens.wait()

    def grad_copy(zc):
        return pltpu.make_async_remote_copy(
            src_ref=gs.at[zc], dst_ref=gr.at[zc], send_sem=send_sem.at[4], recv_sem=g_recv,
            device_id=partner, device_id_type=MESH,
        )

    def grad(zc, carry):
        at = pl.ds(pl.multiple_of(zc * 256, 256), 256)
        g = lax.dot_general(s_v[:, at], c_v[...], ROWS_FIRST, preferred_element_type=F32)
        gs[zc] = g[:, 256:512]
        go[zc] = g[:, 0:256]
        grad_copy(zc).start()
        return carry

    lax.fori_loop(0, 4, grad, 0)

    def relay(k, up):
        left, right = fg.at[c, plus(v, -2), plus(u, -k)], fg.at[c, plus(v, 2), plus(u, -k)]
        arrive(fg.at[c, v, pl.ds(0, 2)], two_recv.at[k])
        if up:
            send(left, left, four_recv, along_v(2), 0)
        else:
            send(right, right, four_recv, along_v(-2), 0)
        send(left, left, three_recv, along_v(1), 0)
        send(right, right, three_recv, along_v(-1), 0)

    def beside(k):
        block = line.at[plus(u, -k)]
        send(block, block, near_recv, along_v(1), 0)
        send(block, block, near_recv, along_v(-1), 0)

    beside(0)
    for k in (1, 7, 2, 6):
        spread(k)
        beside(k)
    relay(0, True)
    for k in (3, 5, 4):
        spread(k)
    for k in (3, 5, 4):
        beside(k)

    lax.fori_loop(4, 8, grad, 0)

    for k in (1, 7, 2, 6):
        relay(k, k < 4)
    for k in (3, 5):
        relay(k, k < 4)
    for k in FAR_FIRST:
        for X in range(2):
            send(mo.at[X], mg.at[X, at_v[X], c], mo_recv.at[1], to_cross(X, k), 0)

    @pl.when(c == 0)
    def _():
        for X in range(2):
            send(mo.at[X], mg.at[X, at_v[X], 0], mo_recv.at[0], partner, 5)

    parts = [pl.ds(4 * i, 4) for i in range(2)]

    def pass_weight(j):
        at = wg.at[c, plus(v, j)]
        send(at, at, wp_recv, partner, 3)

    def weight_step(s):
        a, b = plus(v, 1 - s), plus(v, s - 1)
        up, down = wg.at[c, a], wg.at[c, b]
        for i, part in enumerate(parts):
            if s > 1:
                arrive(wg.at[c, v], w2_recv.at[s - 2, i])
            if s < 4 or i == 0:
                send(up.at[part], up.at[part], w2_recv.at[s - 1, i], along_v(1), 1)
            if s < 4 or i == 1:
                send(down.at[part], down.at[part], w2_recv.at[s - 1, i], along_v(-1), 1)
        pass_weight(1 - s)
        if s > 1:
            pass_weight(s - 1)

    arrive(wg.at[c, v, u, other], w1_recv.at[0])
    arrive(wg.at[c, v, pl.ds(0, 7)], w1_recv.at[1])
    weight_step(1)
    arrive(gr, g_recv)

    def combine(zc, carry):
        high, low = halves(go[zc] + gr[zc])
        for i in range(8):
            a, b = i + c * (zc - i), zc + c * (i - zc)
            gh[a, b] = high[32 * i:32 * i + 32]
            gl[a, b] = low[32 * i:32 * i + 32]
        return carry

    lax.fori_loop(0, 8, combine, 0)

    def project(j):
        f = fg[c, j].reshape(256, 256)
        term = lax.dot_general(f, gh[j].reshape(256, 256), ROWS_FIRST, preferred_element_type=F32)
        term += lax.dot_general(f, gl[j].reshape(256, 256), ROWS_FIRST, preferred_element_type=F32)
        return term.reshape(8, 32, 256)

    def pass_factor(j):
        at = fg.at[c, plus(v, j)]
        send(at, at, fp_recv, partner, 2)

    pass_factor(0)
    pp[...] = project(v)
    arrive(fg.at[c, pl.ds(0, 2)], near_recv)
    pp[...] += project(plus(v, -1))
    pp[...] += project(plus(v, 1))
    pass_factor(-1)
    pass_factor(1)
    arrive(fg.at[c, v, pl.ds(0, 2)], two_recv.at[4])
    pp[...] += project(plus(v, -2))
    pp[...] += project(plus(v, 2))
    pass_factor(-2)
    pass_factor(2)
    arrive(fg.at[c, pl.ds(0, 2)], three_recv)
    pp[...] += project(plus(v, -3))
    pp[...] += project(plus(v, 3))
    arrive(fg.at[c, 0], four_recv)
    pp[...] += project(plus(v, 4))
    for k in FAR_FIRST:
        send(pp.at[plus(u, k)], rb.at[c, u], b2_recv.at[c, k // 4 - k // 5], along_u(k, 1), 0)

    @pl.when(c == 0)
    def _():
        send(pp.at[u], rb.at[0, u], own_recv.at[0], partner, 5)

    pass_factor(-3)
    pass_factor(3)
    pass_factor(4)
    def squared(j, total):
        f = fg[c, j].reshape(256, 256)
        return total + lax.dot_general(f, f, ROWS_FIRST, preferred_element_type=F32)

    gram = lax.fori_loop(0, 8, squared, jnp.zeros((256, 256), F32))
    for i, part in enumerate(thirds(gram)):
        for at in ((0, 256, 1024), (512, 768), (1280,))[i]:
            gm[:, at:at + 256] = part
    weight_step(2)

    @pl.when(c == 1)
    def _():
        for X in (1, 0):
            arrive(rb.at[X, pl.ds(0, 6)], b2_recv.at[X, 0])
            arrive(rb.at[X, 0], b2_recv.at[X, 1])
            if X == 0:
                arrive(rb.at[0, 0], own_recv.at[0])
            total = rb[0, z] if X == 0 else pp[y]
            for k in NEAR_FIRST:
                total += rb[X, plus(at_u[X], -k)]
            mine = ab.at[X, at_v[X]]
            mine[...] = total
            for k in FAR_FIRST:
                send(mine, mine, b3_recv.at[X], to_cross(X, k), 6)
        arrive(mg.at[0, 0], mo_recv.at[0])
        arrive(mg.at[:, pl.ds(0, 7)], mo_recv.at[1])
        for X in range(2):
            for k in range(8):
                for cc in range(2):
                    at = 4 * k + 2 * cc
                    m1c[X, at:at + 2] = mg[X, k, cc, 0:2]
                    m2c[X, at:at + 2] = mg[X, k, cc, 2:4]

    weight_step(3)

    @pl.when(c == 1)
    def _():
        for X in (1, 0):
            arrive(ab.at[X, pl.ds(0, 7)], b3_recv.at[X])
            projected = ab[X, 0]
            for k in range(1, 8):
                projected += ab[X, k]
            first = 0.8 * m1c[X] + 0.2 * projected
            second = 0.9 * m2c[X] + 0.1 * projected * projected
            mine = sm.at[X, at_u[X]]
            mine[...] = first / (jnp.sqrt(second) + 1e-08)
            for k in FAR_FIRST:
                send(mine, mine, c_recv.at[min(k, 8 - k) - 1], to_line(X, k), 6)
            send(mine, mine, own_recv.at[1], partner, 6)
            m1c[X] = first
            m2c[X] = second
        for X in range(2):
            for i in range(2):
                at = 4 * at_v[X] + i
                nst[4 * X + i:4 * X + i + 1] = m1c[X, pl.ds(at, 1)]
                nst[4 * X + 2 + i:4 * X + 3 + i] = m2c[X, pl.ds(at, 1)]
                moments[X, i:i + 1] = m1c[X, pl.ds(at + 2, 1)]
                moments[2 + X, i:i + 1] = m2c[X, pl.ds(at + 2, 1)]
        send(nst, nrx, n_recv, partner, 6)

    weight_step(4)

    @pl.when(c == 0)
    def _():
        arrive(sm.at[0, pl.ds(0, 2)], own_recv.at[1])

    for k in (1, 2, 3, 4):
        pair = (k, -k) if k < 4 else (4,)
        arrive(sm.at[c, pl.ds(0, len(pair))], c_recv.at[k - 1])
        for i in pair:
            at = sm.at[c, plus(u, i)]
            send(at, at, sp_recv, partner, 2)

    small = sm[c].reshape(256, 256)
    high, middle, low = thirds(small)
    spread_small = jnp.concatenate([high, middle, high, middle, low, high], axis=0)
    squares = small * jnp.dot(gm[...], spread_small, preferred_element_type=F32)
    qb[4 * c + x] = jnp.broadcast_to(jnp.sum(squares, keepdims=True), (8, 128))
    mine = qb.at[4 * c + x]
    for k in (2, 1, 3):
        to = lax.rem(x + k, 4)
        send(mine, mine, q_recv, (me, to), 2)
        send(mine, mine, q_recv, (me + 1 - 2 * c, to), 2)
    send(mine, mine, q_recv, partner, 2)

    def expanded(X):
        high, low = halves(sm[X].reshape(256, 256))
        small = jnp.concatenate([high, low], axis=0)

        def expand(j, carry):
            f = fg[X, j].reshape(256, 256)
            value = jnp.dot(jnp.concatenate([f, f], axis=1), small, preferred_element_type=F32)
            full[X, j] = value.reshape(8, 2, 16, 256)
            return carry

        lax.fori_loop(0, 8, expand, 0, unroll=2)

    expanded(c)
    four = wg.at[c, plus(v, 4)]
    for i, part in enumerate(parts):
        arrive(four.at[part], w2_recv.at[3, i])
    pass_weight(4)
    arrive(fg.at[other], fp_recv)
    arrive(sm.at[other, pl.ds(0, 7)], sp_recv)
    expanded(other)
    arrive(qb.at[pl.ds(0, 7)], q_recv)

    @pl.when(c == 0)
    def _():
        arrive(nrx, n_recv)
        for X in range(2):
            moments[X] = nrx[4 * X:4 * X + 2]
            moments[2 + X] = nrx[4 * X + 2:4 * X + 4]

    arrive(wg.at[other], wp_recv)
    sent[4] = 2048

    def drained(group):
        arrive(spare.at[pl.ds(0, sent[group] // 4)], send_sem.at[group])

    for group in range(5):
        drained(group)
    pl.when(c == 0)(lambda: drained(5))
    pl.when(c == 1)(lambda: drained(6))


def write_out(
    entries, full, wg, qb, moments,
    copy_in, copy_out, upd_in, upd_out, new_in, new_out, fst_in, fst_out, snd_in, snd_out,
    copies, rows, sems,
):
    me = lax.axis_index("fs")
    c = lax.rem(me, 2)
    y = lax.rem(lax.div(me, 2), 8)
    z = lax.div(me, 16)
    writes = []

    def write(src, dst):
        writes.append(pltpu.make_async_copy(src, dst, sems.at[len(writes)]))
        writes[-1].start()

    for i, dst in enumerate((fst_in, fst_out, snd_in, snd_out)):
        write(moments.at[i], dst)
    scales = []
    for X in range(2):
        square = ((qb[4 * X] + qb[4 * X + 1]) + qb[4 * X + 2]) + qb[4 * X + 3]
        scale = 1.0 / jnp.sqrt(square[0:1] / entries + 1e-06)
        scales.append(jnp.concatenate([scale, scale], axis=1))

    def line(j, carry):
        for X in range(2):
            update = full[X, j].reshape(256, 256) * scales[X]
            fresh = wg[X, j].reshape(256, 256) - 0.02 * update
            copies[X, j] = fresh.astype(BF16).reshape(8, 32, 256)
            dst = copy_out.at[j] if X else copy_in.at[:, j]
            pltpu.make_async_copy(copies.at[X, j], dst, sems.at[8 + X]).start()
        return carry

    lax.fori_loop(0, 8, line, 0, unroll=2)
    for X in range(2):
        at = (z, y, c) if X else (y, z, c)
        update = full[X, at[0], at[1], at[2]] * scales[X]
        rows[X] = update
        rows[2 + X] = wg[X, at[0], at[1], at[2]] - 0.02 * update
        write(rows.at[X], upd_out if X else upd_in)
        write(rows.at[2 + X], new_out if X else new_in)
    for copy in writes:
        copy.wait()
    for X in range(2):
        pltpu.make_async_copy(copies.at[X], copies.at[X], sems.at[8 + X]).wait()


def on_device(*args):
    shape = jax.ShapeDtypeStruct
    dma = pltpu.SemaphoreType.DMA
    vmem = pltpu.VMEM
    anywhere = pl.BlockSpec(memory_space=pl.ANY)
    scratch = [
        vmem((768, 2048), BF16), vmem((768, 512), BF16),
        vmem((2, 16, 256), BF16), vmem((2, 16, 256), F32), vmem((4, 2, 256), F32),
        vmem((2, 4, 256), F32), vmem((2, 8, 2, 4, 256), F32),
        vmem((2, 32, 256), F32), vmem((2, 32, 256), F32),
        vmem((2, 8, 8, 2, 16, 256), BF16),
        vmem((8, 256, 256), F32), vmem((8, 256, 256), F32), vmem((8, 256, 256), F32), vmem((512, 8, 128), F32),
        vmem((8, 8, 32, 256), BF16), vmem((8, 8, 32, 256), BF16),
        vmem((8, 32, 256), F32), vmem((2, 8, 32, 256), F32),
        vmem((2, 8, 32, 256), F32), vmem((2, 8, 32, 256), F32),
        vmem((8, 256), F32), vmem((8, 256), F32), vmem((256, 1536), BF16),
        dma((5,)), dma((7,)), dma((8,)), dma((2,)), dma((2,)), dma((4, 2)), dma(()), dma((8,)), dma(()), dma(()),
        dma(()), dma(()), dma(()), dma((2, 2)), dma((2,)), dma((2,)), dma((4,)), dma(()), dma(()), dma(()),
    ]
    lines = shape((2, 8, 8, 2, 16, 256), F32)
    mid = pl.pallas_call(
        kernel,
        out_shape=(lines, lines, shape((8, 8, 128), F32), shape((4, 2, 256), F32)),
        in_specs=[pl.BlockSpec(memory_space=pltpu.HBM)] * 11,
        out_specs=(pl.BlockSpec(memory_space=pltpu.VMEM),) * 4,
        scratch_shapes=scratch,
        compiler_params=pltpu.CompilerParams(
            collective_id=0, has_side_effects=True, vmem_limit_bytes=40 * 1024 * 1024
        ),
    )(*(pltpu.with_memory_space_constraint(a, pltpu.HBM) for a in args))
    mid = [pltpu.with_memory_space_constraint(m, pltpu.VMEM) for m in mid]
    whole, row, pair = shape((8, 8, 32, 256), BF16), shape((16, 256), F32), shape((2, 256), F32)
    copy_in, copy_out, *rest = pl.pallas_call(
        functools.partial(write_out, float(2048 * 1024)),
        out_shape=(whole, whole) + (row,) * 4 + (pair,) * 4,
        in_specs=[pl.BlockSpec(memory_space=pltpu.VMEM)] * 4,
        out_specs=(anywhere,) * 10,
        scratch_shapes=[vmem((2, 8, 8, 32, 256), BF16), vmem((4, 16, 256), F32), dma((10,))],
        compiler_params=pltpu.CompilerParams(vmem_limit_bytes=16 * 1024 * 1024),
    )(*mid)
    return (*rest[:4], copy_in.reshape(2048, 256), copy_out.reshape(2048, 256), *rest[4:])


def solution(mesh):
    both, rows, columns = P("fs", "tp"), P("fs", None), P(None, "tp")
    return jax.shard_map(
        on_device,
        mesh=mesh,
        in_specs=(rows, both, both, rows, rows) + (both,) * 6,
        out_specs=(both,) * 4 + (columns,) * 2 + (both,) * 4,
        check_vma=False,
    )
```
